256 devices in a mesh: grp: 2 (over y), fs: 16 (over z), tp: 8 (over x, core).
Axes of the slice: x: 4, y: 2, z: 16, core: 2. Of those that a mesh axis runs over, the one named last changes fastest.
The devices are a block of a 4x16x16 slice.
Arguments:
- layer_input: bfloat16 [12288, 2048], P(('grp', 'fs'), 'tp'), parts along dimension 0, may hold values from -6 to 6
- first_gain: bfloat16 [1, 2048], P(None, 'tp'), may hold values from 0.099609375 to 1.8984375
- ffn_gate_w: bfloat16 [2048, 6144], P('fs', 'tp'), may hold values from -0.125 to 0.125
- ffn_up_w: bfloat16 [2048, 6144], P('fs', 'tp'), may hold values from -0.125 to 0.125
- ffn_down_w: bfloat16 [6144, 2048], P('tp', 'fs'), may hold values from -0.078125 to 0.078125
- mixer_gain: bfloat16 [1, 2048], P(None, 'tp'), may hold values from 0.099609375 to 1.8984375
- pool_in_w: bfloat16 [2048, 1024], P('fs', 'tp'), may hold values from -0.125 to 0.125
- mixer_gate_w: bfloat16 [2048, 2048], P('fs', 'tp'), may hold values from -0.125 to 0.125
- group_mix_w: bfloat16 [8, 128, 128], P('tp'), may hold values from -0.5 to 0.5
- pool_scale: float32 [1, 1024], P(None, 'tp'), may hold values from 0.1 to 1.9
- mixer_out_w: bfloat16 [1024, 2048], P('tp', 'fs'), may hold values from -0.1875 to 0.1875
- second_gain: bfloat16 [1, 2048], P(None, 'tp'), may hold values from 0.099609375 to 1.8984375
Outputs:
- layer_output: bfloat16 [12288, 2048], P(('grp', 'fs'), 'tp'), parts along dimension 0
The draws below stay inside these ranges and needn't reach their ends.
There are 2 independent parts, one for each index of `grp`. The reference program is written for one: setup_inputs(seed, part) draws one part's arguments, and reference() takes and returns one part's arrays. A program takes and returns all parts, laid end to end along the dimension named above; an argument that names none is the same for every part. Nothing has to cross between parts.
All inputs are finite; a program needn't handle non-finite values.
Results may differ from the reference program's by a relative error of at most 0.015.
Values may be sent and summed in bfloat16 or wider, within the bound.
A program may use at most 64 MiB of HBM per device.

```python
import jax
import jax.numpy as jnp
from jax import lax

D = 2048
FF = 6144
BW = 1024
GW = 128
GROUPS = 8
TOK_DEV = 384
TOKENS = 6144
N_FS = 16
N_TP = 8


def steps_of(key, dims, split, low, top_value):
    factor_of = 1.0
    for position, shards_of in split:
        draws = jax.random.uniform(jax.random.fold_in(jax.random.fold_in(key, 6), position), (shards_of,), jnp.float32, low / len(split), top_value / len(split))
        factor_of = factor_of * jnp.repeat(jnp.exp(draws), dims[position] // shards_of).reshape((-1,) + (1,) * (len(dims) - 1 - position))
    return factor_of


def noise(rng, extent, scale, bound, shards=(), kind=jnp.bfloat16):
    drawn = jax.random.normal(rng, extent, jnp.float32) * scale
    if len(shards) > 0:
        drawn = steps_of(rng, extent, shards, -0.22, 0.18) * drawn
    return jnp.clip(drawn, min=-bound, max=bound).astype(kind)


def setup_inputs(seed: int = 0, part: int = 0) -> dict:
    splits = jax.random.split(jax.random.key(seed), 13)
    part_keys = jax.random.split(jax.random.fold_in(splits[12], part), 13)
    layer_input = noise(part_keys[0], (TOKENS, D), 1.0, 6.0, ((0, 16), (1, 8)))
    first_gain = jnp.clip(1.0 + 0.18 * jax.random.normal(splits[1], (1, D), jnp.float32), 0.099609375, 1.8984375).astype(jnp.bfloat16)
    ffn_gate_w = noise(splits[2], (D, FF), D ** -0.5, 0.125, ((0, 16), (1, 8)))
    ffn_up_w = noise(splits[3], (D, FF), D ** -0.5, 0.125, ((0, 16), (1, 8)))
    ffn_down_w = noise(splits[4], (FF, D), FF ** -0.5, 0.078125, ((0, 8), (1, 16)))
    mixer_gain = jnp.clip(1.0 + 0.18 * jax.random.normal(splits[5], (1, D), jnp.float32), 0.099609375, 1.8984375).astype(jnp.bfloat16)
    pool_in_w = noise(splits[6], (D, BW), D ** -0.5, 0.125, ((0, 16), (1, 8)))
    mixer_gate_w = noise(splits[7], (D, D), D ** -0.5, 0.125, ((0, 16), (1, 8)))
    group_mix_w = noise(splits[8], (GROUPS, GW, GW), GW ** -0.5, 0.5, ((0, 8),))
    pool_scale = jnp.clip(1.0 + 0.18 * jax.random.normal(splits[9], (1, BW), jnp.float32), 0.1, 1.9)
    mixer_out_w = noise(splits[10], (BW, D), BW ** -0.5, 0.1875, ((0, 8), (1, 16)))
    second_gain = jnp.clip(1.0 + 0.18 * jax.random.normal(splits[11], (1, D), jnp.float32), 0.099609375, 1.8984375).astype(jnp.bfloat16)
    return dict(layer_input=layer_input, first_gain=first_gain, ffn_gate_w=ffn_gate_w, ffn_up_w=ffn_up_w, ffn_down_w=ffn_down_w, mixer_gain=mixer_gain, pool_in_w=pool_in_w, mixer_gate_w=mixer_gate_w, group_mix_w=group_mix_w, pool_scale=pool_scale, mixer_out_w=mixer_out_w, second_gain=second_gain)


def norm_rows(values, gain):
    widened = values.astype(jnp.float32)
    scaled = (widened * gain.astype(jnp.float32)).astype(jnp.bfloat16)
    factor = lax.rsqrt(lax.optimization_barrier(jnp.mean(widened * widened, axis=1, keepdims=True)) + 1e-06)
    return (scaled, factor)

def block_sum(left, right):
    width = left.shape[1] // N_TP
    total = jnp.zeros((left.shape[0], right.shape[1]), jnp.float32)
    for block in range(N_TP):
        partial_value = jnp.dot(left[:, block * width:(block + 1) * width], right[block * width:(block + 1) * width], preferred_element_type=jnp.float32)
        rounded = lax.optimization_barrier(partial_value.astype(jnp.bfloat16))
        total = total + rounded.astype(jnp.float32)
    return total

def feed_forward(values, gain, ffn_gate_w, ffn_up_w, ffn_down_w):
    scaled, factor = norm_rows(values, gain)
    gate_pre = factor * jnp.dot(scaled, ffn_gate_w, preferred_element_type=jnp.float32)
    up_pre = factor * jnp.dot(scaled, ffn_up_w, preferred_element_type=jnp.float32)
    hidden = (jax.nn.silu(gate_pre) * up_pre).astype(jnp.bfloat16)
    return block_sum(hidden, ffn_down_w)

def reference(layer_input, first_gain, ffn_gate_w, ffn_up_w, ffn_down_w, mixer_gain, pool_in_w, mixer_gate_w, group_mix_w, pool_scale, mixer_out_w, second_gain):
    first = (layer_input.astype(jnp.float32) + 0.5 * feed_forward(layer_input, first_gain, ffn_gate_w, ffn_up_w, ffn_down_w)).astype(jnp.bfloat16)
    scaled, factor = norm_rows(first, mixer_gain)
    pool_pre = (factor * jnp.dot(scaled, pool_in_w, preferred_element_type=jnp.float32)).astype(jnp.bfloat16)
    gate_logit = factor * jnp.dot(scaled, mixer_gate_w, preferred_element_type=jnp.float32)
    values = pool_pre.astype(jnp.float32).reshape(N_FS, TOK_DEV, GROUPS, GW)
    running = jnp.cumsum(values, axis=1)
    positions = jnp.arange(TOK_DEV, dtype=jnp.int32)
    windows = 2 ** (1 + jnp.arange(GROUPS, dtype=jnp.int32) % 4)
    chosen = jnp.zeros_like(values)
    for span in (2, 4, 8, 16):
        lagged = jnp.pad(running, ((0, 0), (span, 0), (0, 0), (0, 0)))[:, :TOK_DEV]
        counts = jnp.minimum(positions + 1, span).astype(jnp.float32)[None, :, None, None]
        means = (running - lagged) / counts
        chosen = jnp.where((windows == span)[None, None, :, None], means, chosen)
    trail = (chosen - values).astype(jnp.bfloat16)
    mixed = jnp.einsum('ntgc,gcd->ntgd', trail.astype(jnp.float32), group_mix_w.astype(jnp.float32))
    pooled = (mixed.reshape(TOKENS, BW) * pool_scale).astype(jnp.bfloat16)
    lifted = block_sum(pooled, mixer_out_w)
    second = (first.astype(jnp.float32) + jax.nn.sigmoid(gate_logit) * lifted).astype(jnp.bfloat16)
    result = second.astype(jnp.float32) + 0.5 * feed_forward(second, second_gain, ffn_gate_w, ffn_up_w, ffn_down_w)
    return result.astype(jnp.bfloat16)
```

```python
import functools

import jax
import jax.numpy as jnp
from jax import lax
from jax.experimental import pallas as pl
from jax.experimental.pallas import tpu as pltpu
from jax.sharding import PartitionSpec as P

F32 = jnp.float32
BF16 = jnp.bfloat16
MESH = pl.DeviceIdType.MESH
EPS = 1e-06
RING_X = 4
NEAR = (2, 1, 3, 0)


def remote(src, dst, send, recv, device):
    return pltpu.make_async_remote_copy(
        src_ref=src, dst_ref=dst, send_sem=send, recv_sem=recv, device_id=device, device_id_type=MESH
    )


def kernel(
    n,
    x_hbm, g1_hbm, gate_hbm, up_hbm, down_hbm, gm_hbm, pin_hbm, mg_hbm, mix_hbm, ps_hbm, mo_hbm, g2_hbm,
    out_ref,
    xin, gains, mixw, pscale,
    wgu, wd, wpg, wo,
    acts, squares, factors, hidden, pre, first, second,
    pair_out, pair_in, turn_out, mid_in, last_in, kept, own,
    in_sem,
    zs_sem, zr_sem, ys_sem, yr_sem,
    ags_sem, agr_sem, sqs_sem, sqr_sem, rss_sem, rsr_sem,
):
    rows, width = x_hbm.shape
    half_rows = rows // 2
    tile = rows // 3
    kdim = gate_hbm.shape[0]
    third = gate_hbm.shape[1] // 3
    half_third = third // 2
    tpn = lax.axis_size("tp")
    features = tpn * width

    grp = lax.axis_index("grp")
    fs = lax.axis_index("fs")
    tp = lax.axis_index("tp")
    x = tp // 2
    core = tp % 2
    parity = grp % 2
    mine = 2 * parity
    other = 2 - mine

    z_right = {"fs": lax.rem(fs + 1, n)}
    z_left = {"fs": lax.rem(fs + n - 1, n)}
    z_dev = (z_right, z_left)
    y_dev = {"grp": grp + 1 - 2 * parity}
    partner = {"tp": tp + 1 - 2 * core}
    x_right = {"tp": lax.rem(tp + 2, tpn)}
    x_left = {"tp": lax.rem(tp + tpn - 2, tpn)}

    sent = []

    def begin(copy):
        copy.start()
        sent.append(copy)

    own_rows = pl.ds(pl.multiple_of(fs * kdim, kdim), kdim)
    local = []

    def fetch(src, dst):
        copy = pltpu.make_async_copy(src, dst, in_sem.at[len(local)])
        copy.start()
        local.append(copy)

    for q, ref in enumerate((gate_hbm, up_hbm)):
        for t in range(3):
            fetch(ref.at[:, pl.ds(t * third, third)], wgu.at[q, t, own_rows])
    fetch(x_hbm, xin)
    for k, ref in enumerate((g1_hbm, gm_hbm, g2_hbm)):
        fetch(ref, gains.at[k])
    early = len(local)
    for t in range(3):
        for h in range(2):
            fetch(down_hbm.at[pl.ds(t * third + h * half_third, half_third)], wd.at[t, h, fs])
    fetch(pin_hbm, wpg.at[0, own_rows])
    for t in range(2):
        fetch(mg_hbm.at[:, pl.ds(t * 128, 128)], wpg.at[1 + t, own_rows])
    fetch(mo_hbm, wo.at[fs])
    fetch(mix_hbm, mixw)
    fetch(ps_hbm, pscale)

    barrier = pltpu.get_barrier_semaphore()
    for dev in (z_right, z_left, y_dev):
        pl.semaphore_signal(barrier, inc=1, device_id=dev, device_id_type=MESH)
    for k in range(1, tpn):
        pl.semaphore_signal(barrier, inc=1, device_id={"tp": lax.rem(tp + k, tpn)}, device_id_type=MESH)
    pl.semaphore_wait(barrier, 3 + tpn - 1)

    def shard(d):
        return lax.rem(fs + n + d, n)

    def rows_of(s):
        return pl.ds(pl.multiple_of(s * kdim, kdim), kdim)

    def z_gate(s):
        return wgu.at[0, pl.ds(parity, 2), rows_of(s)]

    def z_up(s):
        return wgu.at[1, pl.ds(parity, 2), rows_of(s)]

    def z_down0(s):
        return wd.at[pl.ds(parity, 2), 0, s]

    def z_down1(s):
        return wd.at[pl.ds(parity, 2), 1, s]

    def z_pool(s):
        return wpg.at[pl.ds(parity, 2), rows_of(s)]

    def z_lift(s):
        return wo.at[s]

    half_n = n // 2
    chains = (z_gate, z_up, z_down0, z_down1, z_pool, z_lift)
    hops = ((half_n, half_n - 1), (half_n - 1, half_n)) * 3

    def y_gu(slot, s):
        return wgu.at[:, slot, rows_of(s)]

    def y_down(slot, s):
        return wd.at[slot, :, s]

    def y_pool(slot, s):
        return wpg.at[slot, rows_of(s)]

    y_kinds = (y_gu, y_down, y_pool)

    def z_send(k, direction, step):
        region = chains[k](shard(-step if direction == 0 else step))
        begin(remote(region, region, zs_sem.at[k, direction, step], zr_sem.at[k, direction, step], z_dev[direction]))

    def z_wait(k, direction, step):
        region = chains[k](shard(-step if direction == 0 else step))
        remote(
            region, region, zs_sem.at[k, direction, step - 1], zr_sem.at[k, direction, step - 1], z_dev[direction]
        ).wait_recv()
        if step < hops[k][direction]:
            z_send(k, direction, step)

    def y_send(kind, d):
        region = y_kinds[kind](mine, shard(d))
        begin(remote(region, region, ys_sem.at[kind, d % n], yr_sem.at[kind, d % n], y_dev))

    def y_wait_all(kind):
        for step in range(1, half_n + 1):
            for d in (-step, step) if step < half_n else (step,):
                region = y_kinds[kind](other, shard(d))
                remote(region, region, ys_sem.at[kind, d % n], yr_sem.at[kind, d % n], y_dev).wait_recv()

    def z_step(ks, kinds, step):
        for k in ks:
            for direction in range(2):
                if step <= hops[k][direction]:
                    z_wait(k, direction, step)
        for kind in kinds:
            for d in (-step, step) if step < half_n else (step,):
                y_send(kind, d)

    def ag_begin(i, values):
        wide = values.astype(F32)
        acts[i, tp] = (wide * gains[i].astype(F32)).astype(BF16)
        sq = wide * wide
        folded = sq[:, :128] + sq[:, 128:]
        squares[i, tp] = jnp.zeros((8, 128), F32)
        for r in range(3):
            squares[i, tp, r:r + 1] = jnp.sum(folded[r * tile:(r + 1) * tile].T, axis=0, keepdims=True)
        block = acts.at[i, tp]
        for h, dev, base in ((0, x_right, 1), (1, x_left, 3), (1, x_right, 1), (0, x_left, 3)):
            part = block.at[pl.ds(h * half_rows, half_rows)]
            begin(remote(part, part, ags_sem.at[i, base + h], agr_sem.at[i, base + h], dev))
        begin(remote(block, block, ags_sem.at[i, 0], agr_sem.at[i, 0], partner))
        for k in range(1, tpn):
            sq_ref = squares.at[i, tp]
            begin(remote(sq_ref, sq_ref, sqs_sem.at[i, k], sqr_sem.at[i, k], {"tp": lax.rem(tp + k, tpn)}))

    def ag_part(i, side, h, other_core=False):
        offset = (RING_X - 1, 1, 2)[side]
        c = 1 - core if other_core else core
        return acts.at[i, 2 * lax.rem(x + offset, RING_X) + c, pl.ds(h * half_rows, half_rows)]

    def ag_near(i):
        for side, h in ((0, 0), (1, 1), (0, 1), (1, 0)):
            part = ag_part(i, side, h)
            k = 1 + 2 * side + h
            remote(part, part, ags_sem.at[i, k], agr_sem.at[i, k], partner).wait_recv()
            if side == h:
                begin(remote(part, part, ags_sem.at[i, 5 + h], agr_sem.at[i, 5 + h], (x_right, x_left)[side]))
            begin(remote(part, part, ags_sem.at[i, 6 + k], agr_sem.at[i, 6 + k], partner))

    def ag_far(i):
        for h in range(2):
            part = ag_part(i, 2, h)
            k = 5 + h
            remote(part, part, ags_sem.at[i, k], agr_sem.at[i, k], partner).wait_recv()
            begin(remote(part, part, ags_sem.at[i, 6 + k], agr_sem.at[i, 6 + k], partner))

    def ag_end(i):
        for k in range(1, tpn):
            sq_ref = squares.at[i, lax.rem(tp + tpn - k, tpn)]
            remote(sq_ref, sq_ref, sqs_sem.at[i, k], sqr_sem.at[i, k], partner).wait_recv()
        total = squares[i, 0]
        for k in range(1, tpn):
            total = total + squares[i, k]
        factor = lax.rsqrt(total * (1.0 / features) + EPS)
        for r in range(3):
            factors[r * tile:(r + 1) * tile] = jnp.broadcast_to(factor[r:r + 1], (128, 128)).T
        block = acts.at[i, tp + 1 - 2 * core]
        remote(block, block, ags_sem.at[i, 0], agr_sem.at[i, 0], partner).wait_recv()
        for side in range(3):
            for h in range(2):
                part = ag_part(i, side, h, True)
                k = 7 + 2 * side + h
                remote(part, part, ags_sem.at[i, k], agr_sem.at[i, k], partner).wait_recv()

    def whole(i):
        return jnp.concatenate([acts[i, k] for k in range(tpn)], axis=1)

    def rs(i, block):
        def at(o, c):
            return 2 * lax.rem(x + o, RING_X) + c

        for k, o in enumerate(NEAR):
            pair_out[i, k] = block(at(o, 1 - core)).astype(BF16)
            begin(remote(pair_out.at[i, k], pair_in.at[i, k], rss_sem.at[i, k], rsr_sem.at[i, k], partner))

        def paired(k):
            product = block(at(NEAR[k], core))
            remote(pair_out.at[i, k], pair_in.at[i, k], rss_sem.at[i, k], rsr_sem.at[i, k], partner).wait_recv()
            return product + pair_in[i, k].astype(F32)

        low = pl.ds(0, half_rows)
        high = pl.ds(half_rows, half_rows)
        turn_out[i, 0] = paired(0).astype(BF16)
        begin(remote(turn_out.at[i, 0, low], mid_in.at[i, 0], rss_sem.at[i, 4], rsr_sem.at[i, 4], x_right))
        begin(remote(turn_out.at[i, 0, high], mid_in.at[i, 1], rss_sem.at[i, 5], rsr_sem.at[i, 5], x_left))
        right = paired(1)
        turn_out[i, 1, half_rows:] = right[half_rows:].astype(BF16)
        begin(remote(turn_out.at[i, 1, high], last_in.at[i, 0, high], rss_sem.at[i, 7], rsr_sem.at[i, 7], x_right))
        kept[0] = right[:half_rows]
        left = paired(2)
        turn_out[i, 2, :half_rows] = left[:half_rows].astype(BF16)
        begin(remote(turn_out.at[i, 2, low], last_in.at[i, 1, low], rss_sem.at[i, 8], rsr_sem.at[i, 8], x_left))
        kept[1] = left[half_rows:]
        own[...] = paired(3)
        remote(turn_out.at[i, 0, low], mid_in.at[i, 0], rss_sem.at[i, 4], rsr_sem.at[i, 4], x_right).wait_recv()
        turn_out[i, 1, :half_rows] = (kept[0] + mid_in[i, 0].astype(F32)).astype(BF16)
        begin(remote(turn_out.at[i, 1, low], last_in.at[i, 0, low], rss_sem.at[i, 6], rsr_sem.at[i, 6], x_right))
        remote(turn_out.at[i, 0, high], mid_in.at[i, 1], rss_sem.at[i, 5], rsr_sem.at[i, 5], x_left).wait_recv()
        turn_out[i, 2, half_rows:] = (kept[1] + mid_in[i, 1].astype(F32)).astype(BF16)
        begin(remote(turn_out.at[i, 2, high], last_in.at[i, 1, high], rss_sem.at[i, 9], rsr_sem.at[i, 9], x_left))
        for k, side, part in ((7, 0, high), (8, 1, low), (6, 0, low), (9, 1, high)):
            ref = last_in.at[i, side, part]
            remote(ref, ref, rss_sem.at[i, k], rsr_sem.at[i, k], x_right).wait_recv()
        return own[...] + last_in[i, 0].astype(F32) + last_in[i, 1].astype(F32)

    def gu(i, t):
        scaled = whole(i)
        for q in range(2):
            pre[q] = jnp.dot(scaled, wgu[q, t], preferred_element_type=F32)
        for s in range(third // 128):
            cols = slice(s * 128, (s + 1) * 128)
            gate = factors[...] * pre[0, :, cols]
            up = factors[...] * pre[1, :, cols]
            hidden[:, t * third + s * 128:t * third + (s + 1) * 128] = (gate / (1.0 + jnp.exp(-gate)) * up).astype(BF16)

    def down_block(j):
        parts = []
        for t in range(3):
            for h in range(2):
                parts.append(jnp.concatenate([wd[t, h, 2 * j], wd[t, h, 2 * j + 1]], axis=1))
        return jnp.dot(hidden[...], jnp.concatenate(parts, axis=0), preferred_element_type=F32)

    for copy in local[:early]:
        copy.wait()
    gu_ks, late_ks = (0, 1), (2, 3, 4, 5)
    for k in gu_ks:
        for direction in range(2):
            z_send(k, direction, 0)
    ag_begin(0, xin[...])
    for copy in local[early:]:
        copy.wait()
    for step in range(1, half_n + 1):
        if step == half_n:
            for k in late_ks:
                for direction in range(2):
                    z_send(k, direction, 0)
        z_step(gu_ks, (0,), step)
        if step == 1:
            ag_near(0)
        if step == 2:
            ag_far(0)
        if step == 3:
            ag_end(0)
    for step in range(1, half_n + 1):
        z_step(late_ks, (1, 2), step)
        if step == 1:
            y_wait_all(0)
        if 2 <= step < 5:
            gu(0, step - 2)
    y_wait_all(1)
    total = rs(0, down_block)
    first[...] = (xin[...].astype(F32) + 0.5 * total).astype(BF16)
    ag_begin(1, first[...])
    ag_near(1)
    ag_far(1)
    y_wait_all(2)
    ag_end(1)

    scaled = whole(1)
    weights = jnp.concatenate([wpg[t] for t in range(3)], axis=1)
    sums = jnp.dot(scaled, weights, preferred_element_type=F32)
    pool_pre = (factors[...] * sums[:, :128]).astype(BF16)
    for s in range(2):
        logit = factors[...] * sums[:, (1 + s) * 128:(2 + s) * 128]
        pre[0, :, s * 128:(s + 1) * 128] = 1.0 / (1.0 + jnp.exp(-logit))
    values = pool_pre.astype(F32)
    position = lax.broadcasted_iota(jnp.int32, (rows, 128), 0)
    window_id = lax.rem(tp, 4)
    running = values
    chosen = values
    for w in range(4):
        span = 1 << w
        lagged = jnp.where(position >= span, pltpu.roll(running, span, 0), 0.0)
        running = running + lagged
        counts = jnp.minimum(position + 1, 2 * span).astype(F32)
        chosen = jnp.where(window_id == w, running / counts, chosen)
    trail = (chosen - values).astype(BF16)
    mixed = jnp.dot(trail, mixw[0], preferred_element_type=F32)
    hidden[:, :128] = (mixed * pscale[...]).astype(BF16)

    def lift_block(j):
        both = jnp.concatenate([wo[2 * j], wo[2 * j + 1]], axis=1)
        return jnp.dot(hidden[:, :128], both, preferred_element_type=F32)

    total = rs(1, lift_block)
    second[...] = (first[...].astype(F32) + pre[0] * total).astype(BF16)
    ag_begin(2, second[...])
    ag_near(2)
    ag_far(2)
    ag_end(2)
    for t in range(3):
        gu(2, t)
    total = rs(2, down_block)
    out_ref[...] = (second[...].astype(F32) + 0.5 * total).astype(BF16)
    for copy in sent:
        copy.wait_send()


def per_device(n, tpn, *arrays):
    x, gate = arrays[0], arrays[2]
    rows, width = x.shape
    kdim, ff = gate.shape
    third = ff // 3
    vmem = pltpu.VMEM
    dma = pltpu.SemaphoreType.DMA
    half_n = n // 2
    any_spec = pl.BlockSpec(memory_space=pl.ANY)
    return pl.pallas_call(
        functools.partial(kernel, n),
        out_shape=jax.ShapeDtypeStruct((rows, width), BF16),
        in_specs=[any_spec] * len(arrays),
        out_specs=pl.BlockSpec(memory_space=pltpu.VMEM),
        scratch_shapes=[
            vmem((rows, width), BF16),
            vmem((3, 1, width), BF16),
            vmem((1, 128, 128), BF16),
            vmem((1, 128), F32),
            vmem((2, 3, n * kdim, third), BF16),
            vmem((3, 2, n, third // 2, 128), BF16),
            vmem((3, n * kdim, 128), BF16),
            vmem((n, 128, 128), BF16),
            vmem((3, tpn, rows, width), BF16),
            vmem((3, tpn, 8, 128), F32),
            vmem((rows, 128), F32),
            vmem((rows, ff), BF16),
            vmem((2, rows, third), F32),
            vmem((rows, width), BF16),
            vmem((rows, width), BF16),
            vmem((3, 4, rows, width), BF16),
            vmem((3, 4, rows, width), BF16),
            vmem((3, 3, rows, width), BF16),
            vmem((3, 2, rows // 2, width), BF16),
            vmem((3, 2, rows, width), BF16),
            vmem((2, rows // 2, width), F32),
            vmem((rows, width), F32),
            dma((24,)),
            dma((6, 2, half_n)),
            dma((6, 2, half_n)),
            dma((3, n)),
            dma((3, n)),
            dma((3, 13)),
            dma((3, 13)),
            dma((3, tpn)),
            dma((3, tpn)),
            dma((3, 10)),
            dma((3, 10)),
        ],
        compiler_params=pltpu.CompilerParams(
            collective_id=0, has_side_effects=True, vmem_limit_bytes=60 * 1024 * 1024
        ),
    )(*arrays)


def solution(mesh):
    return jax.shard_map(
        functools.partial(per_device, mesh.shape["fs"], mesh.shape["tp"]),
        mesh=mesh,
        in_specs=(
            P(("grp", "fs"), "tp"),
            P(None, "tp"),
            P("fs", "tp"),
            P("fs", "tp"),
            P("tp", "fs"),
            P(None, "tp"),
            P("fs", "tp"),
            P("fs", "tp"),
            P("tp", None, None),
            P(None, "tp"),
            P("tp", "fs"),
            P(None, "tp"),
        ),
        out_specs=P(("grp", "fs"), "tp"),
        check_vma=False,
    )
```

```python
import functools

import jax
import jax.numpy as jnp
from jax import lax
from jax.experimental import pallas as pl
from jax.experimental.pallas import tpu as pltpu
from jax.sharding import PartitionSpec as P

F32 = jnp.float32
BF16 = jnp.bfloat16
MESH = pl.DeviceIdType.MESH
EPS = 1e-06
RING_X = 4
NEAR = (2, 1, 3, 0)
BATCH = (((1, -1), (2, -2)), ((3, -3), (4, -4)), ((5, -5), (6, -6)), ((7, -7), (0, 8)))


def remote(src, dst, send, recv, device):
    return pltpu.make_async_remote_copy(
        src_ref=src, dst_ref=dst, send_sem=send, recv_sem=recv, device_id=device, device_id_type=MESH
    )


def kernel(
    n,
    x_hbm, g1_hbm, gate_hbm, up_hbm, down_hbm, gm_hbm, pin_hbm, mg_hbm, mix_hbm, ps_hbm, mo_hbm, g2_hbm,
    out_ref,
    xin, gains, mixw, pscale,
    wgu, wd, wpg, wo,
    acts, squares, factors, hidden, pre, first, second,
    part, gp_out, gp_in, gt_out, gm_in, gl_in, fall, first_all, scaled_all, sq_sum,
    pair_out, pair_in, turn_out, mid_in, last_in, kept, own,
    in_sem,
    zs_sem, zr_sem, ys_sem, yr_sem,
    ags_sem, agr_sem, sqs_sem, sqr_sem, rss_sem, rsr_sem, gs_sem, gr_sem,
):
    rows, width = x_hbm.shape
    half_rows = rows // 2
    tile = rows // 3
    kdim = gate_hbm.shape[0]
    third = gate_hbm.shape[1] // 3
    half_third = third // 2
    tpn = lax.axis_size("tp")
    features = tpn * width

    grp = lax.axis_index("grp")
    fs = lax.axis_index("fs")
    tp = lax.axis_index("tp")
    x = tp // 2
    core = tp % 2
    parity = grp % 2
    mine = 2 * parity
    other = 2 - mine

    z_right = {"fs": lax.rem(fs + 1, n)}
    z_left = {"fs": lax.rem(fs + n - 1, n)}
    z_dev = (z_right, z_left)
    y_dev = {"grp": grp + 1 - 2 * parity}
    partner = {"tp": tp + 1 - 2 * core}
    x_right = {"tp": lax.rem(tp + 2, tpn)}
    x_left = {"tp": lax.rem(tp + tpn - 2, tpn)}

    sent = []

    def begin(copy):
        copy.start()
        sent.append(copy)

    own_rows = pl.ds(pl.multiple_of(fs * kdim, kdim), kdim)
    local = []

    def fetch(src, dst):
        copy = pltpu.make_async_copy(src, dst, in_sem.at[len(local)])
        copy.start()
        local.append(copy)

    for q, ref in enumerate((gate_hbm, up_hbm)):
        for t in range(3):
            fetch(ref.at[:, pl.ds(t * third, third)], wgu.at[q, t, own_rows])
    fetch(x_hbm, xin)
    for k, ref in enumerate((g1_hbm, gm_hbm, g2_hbm)):
        fetch(ref, gains.at[tp, k])
    early = len(local)
    for t in range(3):
        for h in range(2):
            fetch(down_hbm.at[pl.ds(t * third + h * half_third, half_third)], wd.at[t, h, fs])
    fetch(pin_hbm, wpg.at[0, own_rows])
    for t in range(2):
        fetch(mg_hbm.at[:, pl.ds(t * 128, 128)], wpg.at[1 + t, own_rows])
    fetch(mo_hbm, wo.at[fs])
    fetch(mix_hbm, mixw)
    fetch(ps_hbm, pscale)

    barrier = pltpu.get_barrier_semaphore()
    for dev in (z_right, z_left, y_dev):
        pl.semaphore_signal(barrier, inc=1, device_id=dev, device_id_type=MESH)
    for k in range(1, tpn):
        pl.semaphore_signal(barrier, inc=1, device_id={"tp": lax.rem(tp + k, tpn)}, device_id_type=MESH)
    pl.semaphore_wait(barrier, 3 + tpn - 1)

    def shard(d):
        return lax.rem(fs + n + d, n)

    def rows_of(s):
        return pl.ds(pl.multiple_of(s * kdim, kdim), kdim)

    def z_gate(s):
        return wgu.at[0, pl.ds(parity, 2), rows_of(s)]

    def z_up(s):
        return wgu.at[1, pl.ds(parity, 2), rows_of(s)]

    def z_down0(s):
        return wd.at[pl.ds(parity, 2), 0, s]

    def z_down1(s):
        return wd.at[pl.ds(parity, 2), 1, s]

    def z_pool(s):
        return wpg.at[pl.ds(parity, 2), rows_of(s)]

    def z_lift(s):
        return wo.at[s]

    half_n = n // 2
    chains = (z_gate, z_up, z_down0, z_down1, z_pool, z_lift)
    hops = ((half_n, half_n - 1), (half_n - 1, half_n)) * 3

    def y_gu(slot, s):
        return wgu.at[:, slot, rows_of(s)]

    def y_down(slot, s):
        return wd.at[slot, :, s]

    def y_pool(slot, s):
        return wpg.at[slot, rows_of(s)]

    y_kinds = (y_gu, y_down, y_pool)

    def z_send(k, direction, step):
        region = chains[k](shard(-step if direction == 0 else step))
        begin(remote(region, region, zs_sem.at[k, direction, step], zr_sem.at[k, direction, step], z_dev[direction]))

    def z_wait(k, direction, step):
        region = chains[k](shard(-step if direction == 0 else step))
        remote(
            region, region, zs_sem.at[k, direction, step - 1], zr_sem.at[k, direction, step - 1], z_dev[direction]
        ).wait_recv()
        if step < hops[k][direction]:
            z_send(k, direction, step)

    def y_send(kind, d):
        region = y_kinds[kind](mine, shard(d))
        begin(remote(region, region, ys_sem.at[kind, d % n], yr_sem.at[kind, d % n], y_dev))

    def y_wait(kind, d):
        region = y_kinds[kind](other, shard(d))
        remote(region, region, ys_sem.at[kind, d % n], yr_sem.at[kind, d % n], y_dev).wait_recv()

    def y_wait_all(kind):
        for step in range(1, half_n + 1):
            for d in (-step, step) if step < half_n else (step,):
                y_wait(kind, d)

    def z_step(ks, kinds, step):
        for k in ks:
            for direction in range(2):
                if step <= hops[k][direction]:
                    z_wait(k, direction, step)
        for kind in kinds:
            for d in (-step, step) if step < half_n else (step,):
                y_send(kind, d)

    def ag_begin(i, values):
        if i == 0:
            acts[i, tp] = values
        else:
            wide = values.astype(F32)
            acts[i, tp] = (wide * gains[tp, i].astype(F32)).astype(BF16)
            sq = wide * wide
            folded = sq[:, :128] + sq[:, 128:]
            squares[tp] = jnp.zeros((8, 128), F32)
            for r in range(3):
                squares[tp, r:r + 1] = jnp.sum(folded[r * tile:(r + 1) * tile].T, axis=0, keepdims=True)
        block = acts.at[i, tp]
        for h, dev, base in ((0, x_right, 1), (1, x_left, 3), (1, x_right, 1), (0, x_left, 3)):
            part = block.at[pl.ds(h * half_rows, half_rows)]
            begin(remote(part, part, ags_sem.at[i, base + h], agr_sem.at[i, base + h], dev))
        begin(remote(block, block, ags_sem.at[i, 0], agr_sem.at[i, 0], partner))
        for k in range(1, tpn):
            sq_ref = gains.at[tp] if i == 0 else squares.at[tp]
            begin(remote(sq_ref, sq_ref, sqs_sem.at[i, k], sqr_sem.at[i, k], {"tp": lax.rem(tp + k, tpn)}))

    def ag_part(i, side, h, other_core=False):
        offset = (RING_X - 1, 1, 2)[side]
        c = 1 - core if other_core else core
        return acts.at[i, 2 * lax.rem(x + offset, RING_X) + c, pl.ds(h * half_rows, half_rows)]

    def ag_near(i):
        for side, h in ((0, 0), (1, 1), (0, 1), (1, 0)):
            part = ag_part(i, side, h)
            k = 1 + 2 * side + h
            remote(part, part, ags_sem.at[i, k], agr_sem.at[i, k], partner).wait_recv()
            if side == h:
                begin(remote(part, part, ags_sem.at[i, 5 + h], agr_sem.at[i, 5 + h], (x_right, x_left)[side]))
            begin(remote(part, part, ags_sem.at[i, 6 + k], agr_sem.at[i, 6 + k], partner))

    def ag_far(i):
        for h in range(2):
            part = ag_part(i, 2, h)
            k = 5 + h
            remote(part, part, ags_sem.at[i, k], agr_sem.at[i, k], partner).wait_recv()
            begin(remote(part, part, ags_sem.at[i, 6 + k], agr_sem.at[i, 6 + k], partner))

    def ag_end(i):
        for k in range(1, tpn):
            sq_ref = (gains if i == 0 else squares).at[lax.rem(tp + tpn - k, tpn)]
            remote(sq_ref, sq_ref, sqs_sem.at[i, k], sqr_sem.at[i, k], partner).wait_recv()
        if i > 0:
            total = squares[0]
            for k in range(1, tpn):
                total = total + squares[k]
            factor = lax.rsqrt(total * (1.0 / features) + EPS)
            for r in range(3):
                factors[r * tile:(r + 1) * tile] = jnp.broadcast_to(factor[r:r + 1], (128, 128)).T
        block = acts.at[i, tp + 1 - 2 * core]
        remote(block, block, ags_sem.at[i, 0], agr_sem.at[i, 0], partner).wait_recv()
        for side in range(3):
            for h in range(2):
                part = ag_part(i, side, h, True)
                k = 7 + 2 * side + h
                remote(part, part, ags_sem.at[i, k], agr_sem.at[i, k], partner).wait_recv()

    def whole(i):
        return jnp.concatenate([acts[i, k] for k in range(tpn)], axis=1)

    def factors_from_sum():
        total = jnp.sum(sq_sum[...], axis=1, keepdims=True)
        factors[...] = jnp.broadcast_to(lax.rsqrt(total * (1.0 / features) + EPS), (rows, 128))

    def scale_input(k):
        wide = acts[0, k].astype(F32)
        acts[1, k] = (wide * gains[k, 0].astype(F32)).astype(BF16)
        sq = wide * wide
        both = sq[:, :128] + sq[:, 128:]
        sq_sum[...] = both if k == 0 else sq_sum[...] + both

    chunk = rows // tpn

    def rows_at(o, c):
        return pl.ds(pl.multiple_of((2 * lax.rem(x + o, RING_X) + c) * chunk, 16), chunk)

    def g_remote(g, src, dst, k, dev):
        return remote(src, dst, gs_sem.at[g, k], gr_sem.at[g, k], dev)

    def g_wait(g, ref, k):
        g_remote(g, ref, ref, k, partner).wait_recv()

    def paired_sum(g, k, h):
        return part[g, h, rows_at(NEAR[k], core)] + gp_in[g, k, h].astype(F32)

    x_dev = (x_right, x_left)

    def g_multiply(g):
        for h in range(2):
            for d in BATCH[g][h]:
                if d != 0:
                    y_wait(1, d)
        for h in range(2):
            d0, d1 = BATCH[g][h]
            parts = []
            for t in range(3):
                for q in range(2):
                    parts.append(jnp.concatenate([wd[t, q, shard(d0)], wd[t, q, shard(d1)]], axis=1))
            part[g, h] = jnp.dot(hidden[...], jnp.concatenate(parts, axis=0), preferred_element_type=F32)
        for k, o in enumerate(NEAR):
            for h in range(2):
                gp_out[g, k, h] = part[g, h, rows_at(o, 1 - core)].astype(BF16)
        begin(g_remote(g, gp_out.at[g], gp_in.at[g], 0, partner))

    def g_pair(g):
        g_wait(g, gp_in.at[g], 0)
        for h in range(2):
            gt_out[g, 0, h] = paired_sum(g, 0, h).astype(BF16)
            begin(g_remote(g, gt_out.at[g, 0, h], gm_in.at[g, h], 1 + h, x_dev[h]))
        for side in range(2):
            gt_out[g, 1 + side, 1 - side] = paired_sum(g, 1 + side, 1 - side).astype(BF16)
            begin(g_remote(
                g, gt_out.at[g, 1 + side, 1 - side], gl_in.at[g, side, 1 - side], 3 + 2 * side + 1 - side, x_dev[side]
            ))

    def g_turn(g):
        for side in range(2):
            g_wait(g, gm_in.at[g, side], 1 + side)
            gt_out[g, 1 + side, side] = (paired_sum(g, 1 + side, side) + gm_in[g, side].astype(F32)).astype(BF16)
            begin(g_remote(g, gt_out.at[g, 1 + side, side], gl_in.at[g, side, side], 3 + 3 * side, x_dev[side]))

    def g_first(g):
        for side in range(2):
            for h in range(2):
                g_wait(g, gl_in.at[g, side, h], 3 + 2 * side + h)
        for h in range(2):
            total = paired_sum(g, 3, h) + gl_in[g, 0, h].astype(F32) + gl_in[g, 1, h].astype(F32)
            for e in range(2):
                b = shard(BATCH[g][h][e])
                both = acts[0, b // 2, pl.ds(pl.multiple_of(tp * chunk, 16), chunk)].astype(F32)
                base = jnp.where(b % 2 == 1, both[:, 128:], both[:, :128])
                cols = slice(e * 128, (e + 1) * 128)
                fall[g, tp, h, :, cols] = (base + 0.5 * total[:, cols]).astype(BF16)
        block = fall.at[g, tp]
        begin(g_remote(g, block, block, 8, x_right))
        begin(g_remote(g, block, block, 9, x_left))
        begin(g_remote(g, block, block, 7, partner))

    def fall_of(g, o, c):
        return fall.at[g, 2 * lax.rem(x + o, RING_X) + c]

    def g_near(g):
        for side in range(2):
            block = fall_of(g, (RING_X - 1, 1)[side], core)
            g_wait(g, block, 8 + side)
            begin(g_remote(g, block.at[side], block.at[side], 10 + side, x_dev[side]))
            begin(g_remote(g, block, block, 12 + side, partner))

    def g_far(g):
        block = fall_of(g, 2, core)
        for h in range(2):
            g_wait(g, block.at[h], 10 + h)
            begin(g_remote(g, block.at[h], block.at[h], 14 + h, partner))

    def g_end(g):
        g_wait(g, fall_of(g, 0, 1 - core), 7)
        g_wait(g, fall_of(g, RING_X - 1, 1 - core), 12)
        g_wait(g, fall_of(g, 1, 1 - core), 13)
        for h in range(2):
            g_wait(g, fall_of(g, 2, 1 - core).at[h], 14 + h)
        for h in range(2):
            for e in range(2):
                b = shard(BATCH[g][h][e])
                value = jnp.concatenate([fall[g, k, h, :, e * 128:(e + 1) * 128] for k in range(tpn)], axis=0)
                first_all[b] = value
                wide = value.astype(F32)
                gain = gains[b // 2, 1].astype(F32)
                gain = jnp.where(b % 2 == 1, gain[:, 128:], gain[:, :128])
                scaled_all[b] = (wide * gain).astype(BF16)
                sq = wide * wide
                sq_sum[...] = sq if g == h == e == 0 else sq_sum[...] + sq

    def rs(i, block):
        def at(o, c):
            return 2 * lax.rem(x + o, RING_X) + c

        for k, o in enumerate(NEAR):
            pair_out[i, k] = block(at(o, 1 - core)).astype(BF16)
            begin(remote(pair_out.at[i, k], pair_in.at[i, k], rss_sem.at[i, k], rsr_sem.at[i, k], partner))

        def paired(k):
            product = block(at(NEAR[k], core))
            remote(pair_out.at[i, k], pair_in.at[i, k], rss_sem.at[i, k], rsr_sem.at[i, k], partner).wait_recv()
            return product + pair_in[i, k].astype(F32)

        low = pl.ds(0, half_rows)
        high = pl.ds(half_rows, half_rows)
        turn_out[i, 0] = paired(0).astype(BF16)
        begin(remote(turn_out.at[i, 0, low], mid_in.at[i, 0], rss_sem.at[i, 4], rsr_sem.at[i, 4], x_right))
        begin(remote(turn_out.at[i, 0, high], mid_in.at[i, 1], rss_sem.at[i, 5], rsr_sem.at[i, 5], x_left))
        right = paired(1)
        turn_out[i, 1, half_rows:] = right[half_rows:].astype(BF16)
        begin(remote(turn_out.at[i, 1, high], last_in.at[i, 0, high], rss_sem.at[i, 7], rsr_sem.at[i, 7], x_right))
        kept[0] = right[:half_rows]
        left = paired(2)
        turn_out[i, 2, :half_rows] = left[:half_rows].astype(BF16)
        begin(remote(turn_out.at[i, 2, low], last_in.at[i, 1, low], rss_sem.at[i, 8], rsr_sem.at[i, 8], x_left))
        kept[1] = left[half_rows:]
        own[...] = paired(3)
        remote(turn_out.at[i, 0, low], mid_in.at[i, 0], rss_sem.at[i, 4], rsr_sem.at[i, 4], x_right).wait_recv()
        turn_out[i, 1, :half_rows] = (kept[0] + mid_in[i, 0].astype(F32)).astype(BF16)
        begin(remote(turn_out.at[i, 1, low], last_in.at[i, 0, low], rss_sem.at[i, 6], rsr_sem.at[i, 6], x_right))
        remote(turn_out.at[i, 0, high], mid_in.at[i, 1], rss_sem.at[i, 5], rsr_sem.at[i, 5], x_left).wait_recv()
        turn_out[i, 2, half_rows:] = (kept[1] + mid_in[i, 1].astype(F32)).astype(BF16)
        begin(remote(turn_out.at[i, 2, high], last_in.at[i, 1, high], rss_sem.at[i, 9], rsr_sem.at[i, 9], x_left))
        for k, side, part in ((7, 0, high), (8, 1, low), (6, 0, low), (9, 1, high)):
            ref = last_in.at[i, side, part]
            remote(ref, ref, rss_sem.at[i, k], rsr_sem.at[i, k], x_right).wait_recv()
        return own[...] + last_in[i, 0].astype(F32) + last_in[i, 1].astype(F32)

    def gu(i, t):
        scaled = whole(i)
        for q in range(2):
            pre[q] = jnp.dot(scaled, wgu[q, t], preferred_element_type=F32)
        for s in range(third // 128):
            cols = slice(s * 128, (s + 1) * 128)
            gate = factors[...] * pre[0, :, cols]
            up = factors[...] * pre[1, :, cols]
            hidden[:, t * third + s * 128:t * third + (s + 1) * 128] = (gate / (1.0 + jnp.exp(-gate)) * up).astype(BF16)

    def down_block(j):
        parts = []
        for t in range(3):
            for h in range(2):
                parts.append(jnp.concatenate([wd[t, h, 2 * j], wd[t, h, 2 * j + 1]], axis=1))
        return jnp.dot(hidden[...], jnp.concatenate(parts, axis=0), preferred_element_type=F32)

    for copy in local[:early]:
        copy.wait()
    gu_ks, late_ks = (0, 1), (2, 3, 4, 5)
    for k in gu_ks:
        for direction in range(2):
            z_send(k, direction, 0)
    ag_begin(0, xin[...])
    for copy in local[early:]:
        copy.wait()
    for k in late_ks:
        for direction in range(2):
            z_send(k, direction, 0)
    for step in range(1, half_n + 1):
        z_step(gu_ks, (0,), step)
        if step == 1:
            ag_near(0)
        if step == 2:
            ag_far(0)
        if step == 3:
            ag_end(0)
        if 4 <= step < 8:
            scale_input(2 * step - 8)
            scale_input(2 * step - 7)
    factors_from_sum()
    stages = (g_multiply, g_pair, g_turn, g_first, g_near, g_far, g_end)
    for slot in range(1, 2 * half_n + 1):
        if slot <= half_n:
            z_step((2, 3), (1,), slot)
        else:
            z_step((4, 5), (2,), slot - half_n)
        if slot == 2:
            y_wait_all(0)
        if 2 <= slot < 5:
            gu(1, slot - 2)
        for k, stage in reversed(tuple(enumerate(stages))):
            g = (slot - 4 - k) // 2
            if (slot - 4 - k) % 2 == 0 and 0 <= g < len(BATCH):
                stage(g)
    y_wait_all(2)
    factors_from_sum()
    first[...] = jnp.concatenate([first_all[2 * tp], first_all[2 * tp + 1]], axis=1)

    scaled = jnp.concatenate([scaled_all[b] for b in range(n)], axis=1)
    weights = jnp.concatenate([wpg[t] for t in range(3)], axis=1)
    sums = jnp.dot(scaled, weights, preferred_element_type=F32)
    pool_pre = (factors[...] * sums[:, :128]).astype(BF16)
    for s in range(2):
        logit = factors[...] * sums[:, (1 + s) * 128:(2 + s) * 128]
        pre[0, :, s * 128:(s + 1) * 128] = 1.0 / (1.0 + jnp.exp(-logit))
    values = pool_pre.astype(F32)
    position = lax.broadcasted_iota(jnp.int32, (rows, 128), 0)
    window_id = lax.rem(tp, 4)
    running = values
    chosen = values
    for w in range(4):
        span = 1 << w
        lagged = jnp.where(position >= span, pltpu.roll(running, span, 0), 0.0)
        running = running + lagged
        counts = jnp.minimum(position + 1, 2 * span).astype(F32)
        chosen = jnp.where(window_id == w, running / counts, chosen)
    trail = (chosen - values).astype(BF16)
    mixed = jnp.dot(trail, mixw[0], preferred_element_type=F32)
    hidden[:, :128] = (mixed * pscale[...]).astype(BF16)

    def lift_block(j):
        both = jnp.concatenate([wo[2 * j], wo[2 * j + 1]], axis=1)
        return jnp.dot(hidden[:, :128], both, preferred_element_type=F32)

    total = rs(1, lift_block)
    second[...] = (first[...].astype(F32) + pre[0] * total).astype(BF16)
    ag_begin(2, second[...])
    ag_near(2)
    ag_far(2)
    ag_end(2)
    for t in range(3):
        gu(2, t)
    total = rs(2, down_block)
    out_ref[...] = (second[...].astype(F32) + 0.5 * total).astype(BF16)
    for copy in sent:
        copy.wait_send()


def per_device(n, tpn, *arrays):
    x, gate = arrays[0], arrays[2]
    rows, width = x.shape
    kdim, ff = gate.shape
    third = ff // 3
    chunk = rows // tpn
    vmem = pltpu.VMEM
    dma = pltpu.SemaphoreType.DMA
    half_n = n // 2
    any_spec = pl.BlockSpec(memory_space=pl.ANY)
    return pl.pallas_call(
        functools.partial(kernel, n),
        out_shape=jax.ShapeDtypeStruct((rows, width), BF16),
        in_specs=[any_spec] * len(arrays),
        out_specs=pl.BlockSpec(memory_space=pltpu.VMEM),
        scratch_shapes=[
            vmem((rows, width), BF16),
            vmem((tpn, 3, 1, width), BF16),
            vmem((1, 128, 128), BF16),
            vmem((1, 128), F32),
            vmem((2, 3, n * kdim, third), BF16),
            vmem((3, 2, n, third // 2, 128), BF16),
            vmem((3, n * kdim, 128), BF16),
            vmem((n, 128, 128), BF16),
            vmem((3, tpn, rows, width), BF16),
            vmem((tpn, 8, 128), F32),
            vmem((rows, 128), F32),
            vmem((rows, ff), BF16),
            vmem((2, rows, third), F32),
            vmem((rows, width), BF16),
            vmem((rows, width), BF16),
            vmem((4, 2, rows, width), F32),
            vmem((4, 4, 2, chunk, width), BF16),
            vmem((4, 4, 2, chunk, width), BF16),
            vmem((4, 3, 2, chunk, width), BF16),
            vmem((4, 2, chunk, width), BF16),
            vmem((4, 2, 2, chunk, width), BF16),
            vmem((4, tpn, 2, chunk, width), BF16),
            vmem((n, rows, 128), BF16),
            vmem((n, rows, 128), BF16),
            vmem((rows, 128), F32),
            vmem((3, 4, rows, width), BF16),
            vmem((3, 4, rows, width), BF16),
            vmem((3, 3, rows, width), BF16),
            vmem((3, 2, rows // 2, width), BF16),
            vmem((3, 2, rows, width), BF16),
            vmem((2, rows // 2, width), F32),
            vmem((rows, width), F32),
            dma((24,)),
            dma((6, 2, half_n)),
            dma((6, 2, half_n)),
            dma((3, n)),
            dma((3, n)),
            dma((3, 13)),
            dma((3, 13)),
            dma((3, tpn)),
            dma((3, tpn)),
            dma((3, 10)),
            dma((3, 10)),
            dma((4, 16)),
            dma((4, 16)),
        ],
        compiler_params=pltpu.CompilerParams(
            collective_id=0, has_side_effects=True, vmem_limit_bytes=60 * 1024 * 1024
        ),
    )(*arrays)


def solution(mesh):
    return jax.shard_map(
        functools.partial(per_device, mesh.shape["fs"], mesh.shape["tp"]),
        mesh=mesh,
        in_specs=(
            P(("grp", "fs"), "tp"),
            P(None, "tp"),
            P("fs", "tp"),
            P("fs", "tp"),
            P("tp", "fs"),
            P(None, "tp"),
            P("fs", "tp"),
            P("fs", "tp"),
            P("tp", None, None),
            P(None, "tp"),
            P("tp", "fs"),
            P(None, "tp"),
        ),
        out_specs=P(("grp", "fs"), "tp"),
        check_vma=False,
    )
```

```python
import functools

import jax
import jax.numpy as jnp
from jax import lax
from jax.experimental import pallas as pl
from jax.experimental.pallas import tpu as pltpu
from jax.sharding import PartitionSpec as P

F32 = jnp.float32
BF16 = jnp.bfloat16
MESH = pl.DeviceIdType.MESH
EPS = 1e-06
RING_X = 4
NEAR = (2, 1, 3, 0)
BATCH = (((1, -1), (2, -2)), ((3, -3), (4, -4)), ((5, -5), (6, -6)), ((7, -7), (0, 8)))


def remote(src, dst, send, recv, device):
    return pltpu.make_async_remote_copy(
        src_ref=src, dst_ref=dst, send_sem=send, recv_sem=recv, device_id=device, device_id_type=MESH
    )


def kernel(
    n,
    x_hbm, g1_hbm, gate_hbm, up_hbm, down_hbm, gm_hbm, pin_hbm, mg_hbm, mix_hbm, ps_hbm, mo_hbm, g2_hbm,
    out_ref,
    xin, gains, mixw, pscale,
    wgu, wd, wpg, wo,
    acts, squares, factors, hidden, pre, first, second,
    mixed_in, part, gp_out, gp_in, gt_out, gm_in, gl_in, fall, first_all, scaled_all, sq_sum,
    pair_out, pair_in, turn_out, mid_in, last_in, kept, own,
    in_sem,
    zs_sem, zr_sem, ys_sem, yr_sem,
    ags_sem, agr_sem, sqs_sem, sqr_sem, rss_sem, rsr_sem, gs_sem, gr_sem,
):
    rows, width = x_hbm.shape
    half_rows = rows // 2
    tile = rows // 3
    kdim = gate_hbm.shape[0]
    third = gate_hbm.shape[1] // 3
    half_third = third // 2
    tpn = lax.axis_size("tp")
    features = tpn * width

    grp = lax.axis_index("grp")
    fs = lax.axis_index("fs")
    tp = lax.axis_index("tp")
    x = tp // 2
    core = tp % 2
    parity = grp % 2
    mine = 2 * parity
    other = 2 - mine

    z_right = {"fs": lax.rem(fs + 1, n)}
    z_left = {"fs": lax.rem(fs + n - 1, n)}
    z_dev = (z_right, z_left)
    y_dev = {"grp": grp + 1 - 2 * parity}
    partner = {"tp": tp + 1 - 2 * core}
    x_right = {"tp": lax.rem(tp + 2, tpn)}
    x_left = {"tp": lax.rem(tp + tpn - 2, tpn)}

    sent = []

    def begin(copy):
        copy.start()
        sent.append(copy)

    own_rows = pl.ds(pl.multiple_of(fs * kdim, kdim), kdim)
    local = []

    def fetch(src, dst):
        copy = pltpu.make_async_copy(src, dst, in_sem.at[len(local)])
        copy.start()
        local.append(copy)

    for q, ref in enumerate((gate_hbm, up_hbm)):
        for t in range(3):
            fetch(ref.at[:, pl.ds(t * third, third)], wgu.at[q, t, own_rows])
    fetch(x_hbm, xin)
    for k, ref in enumerate((g1_hbm, gm_hbm, g2_hbm)):
        fetch(ref, gains.at[tp, k])
    early = len(local)
    for t in range(3):
        for h in range(2):
            fetch(down_hbm.at[pl.ds(t * third + h * half_third, half_third)], wd.at[t, h, fs])
    fetch(pin_hbm, wpg.at[0, own_rows])
    for t in range(2):
        fetch(mg_hbm.at[:, pl.ds(t * 128, 128)], wpg.at[1 + t, own_rows])
    fetch(mo_hbm, wo.at[fs])
    fetch(mix_hbm, mixw)
    fetch(ps_hbm, pscale)

    barrier = pltpu.get_barrier_semaphore()
    for dev in (z_right, z_left, y_dev):
        pl.semaphore_signal(barrier, inc=1, device_id=dev, device_id_type=MESH)
    for k in range(1, tpn):
        pl.semaphore_signal(barrier, inc=1, device_id={"tp": lax.rem(tp + k, tpn)}, device_id_type=MESH)
    pl.semaphore_wait(barrier, 3 + tpn - 1)

    def shard(d):
        return lax.rem(fs + n + d, n)

    def rows_of(s):
        return pl.ds(pl.multiple_of(s * kdim, kdim), kdim)

    def z_gate(s):
        return wgu.at[0, pl.ds(parity, 2), rows_of(s)]

    def z_up(s):
        return wgu.at[1, pl.ds(parity, 2), rows_of(s)]

    def z_down(t, q):
        return lambda s: wd.at[parity + t, q, s]

    def z_pool(s):
        return wpg.at[pl.ds(parity, 2), rows_of(s)]

    def z_lift(s):
        return wo.at[s]

    half_n = n // 2
    chains = (z_gate, z_up, z_pool, z_lift, z_down(0, 0), z_down(1, 1), z_down(1, 0), z_down(0, 1))
    hops = ((half_n, half_n - 1), (half_n - 1, half_n)) * 4

    def y_gu(slot, s):
        return wgu.at[:, slot, rows_of(s)]

    def y_down(slot, s):
        return wd.at[slot, :, s]

    def y_pool(slot, s):
        return wpg.at[slot, rows_of(s)]

    y_kinds = (y_gu, y_down, y_pool)

    def z_send(k, direction, step):
        region = chains[k](shard(-step if direction == 0 else step))
        begin(remote(region, region, zs_sem.at[k, direction, step], zr_sem.at[k, direction, step], z_dev[direction]))

    def z_wait(k, direction, step):
        region = chains[k](shard(-step if direction == 0 else step))
        remote(
            region, region, zs_sem.at[k, direction, step - 1], zr_sem.at[k, direction, step - 1], z_dev[direction]
        ).wait_recv()
        if step < hops[k][direction]:
            z_send(k, direction, step)

    def y_send(kind, d):
        region = y_kinds[kind](mine, shard(d))
        begin(remote(region, region, ys_sem.at[kind, d % n], yr_sem.at[kind, d % n], y_dev))

    def y_wait(kind, d):
        region = y_kinds[kind](other, shard(d))
        remote(region, region, ys_sem.at[kind, d % n], yr_sem.at[kind, d % n], y_dev).wait_recv()

    def y_wait_all(kind):
        for step in range(1, half_n + 1):
            for d in (-step, step) if step < half_n else (step,):
                y_wait(kind, d)

    def z_step(ks, kinds, step):
        for k in ks:
            for direction in range(2):
                if step <= hops[k][direction]:
                    z_wait(k, direction, step)
        for kind in kinds:
            for d in (-step, step) if step < half_n else (step,):
                y_send(kind, d)

    def ag_begin(i, values):
        if i == 0:
            acts[i, tp] = values
        else:
            wide = values.astype(F32)
            acts[i, tp] = (wide * gains[tp, i].astype(F32)).astype(BF16)
            sq = wide * wide
            folded = sq[:, :128] + sq[:, 128:]
            squares[tp] = jnp.zeros((8, 128), F32)
            for r in range(3):
                squares[tp, r:r + 1] = jnp.sum(folded[r * tile:(r + 1) * tile].T, axis=0, keepdims=True)
        block = acts.at[i, tp]
        for h, dev, base in ((0, x_right, 1), (1, x_left, 3), (1, x_right, 1), (0, x_left, 3)):
            part = block.at[pl.ds(h * half_rows, half_rows)]
            begin(remote(part, part, ags_sem.at[i, base + h], agr_sem.at[i, base + h], dev))
        begin(remote(block, block, ags_sem.at[i, 0], agr_sem.at[i, 0], partner))
        for k in range(1, tpn):
            sq_ref = gains.at[tp] if i == 0 else squares.at[tp]
            begin(remote(sq_ref, sq_ref, sqs_sem.at[i, k], sqr_sem.at[i, k], {"tp": lax.rem(tp + k, tpn)}))

    def ag_part(i, side, h, other_core=False):
        offset = (RING_X - 1, 1, 2)[side]
        c = 1 - core if other_core else core
        return acts.at[i, 2 * lax.rem(x + offset, RING_X) + c, pl.ds(h * half_rows, half_rows)]

    def ag_near(i):
        for side, h in ((0, 0), (1, 1), (0, 1), (1, 0)):
            part = ag_part(i, side, h)
            k = 1 + 2 * side + h
            remote(part, part, ags_sem.at[i, k], agr_sem.at[i, k], partner).wait_recv()
            if side == h:
                begin(remote(part, part, ags_sem.at[i, 5 + h], agr_sem.at[i, 5 + h], (x_right, x_left)[side]))
            begin(remote(part, part, ags_sem.at[i, 6 + k], agr_sem.at[i, 6 + k], partner))

    def ag_far(i):
        for h in range(2):
            part = ag_part(i, 2, h)
            k = 5 + h
            remote(part, part, ags_sem.at[i, k], agr_sem.at[i, k], partner).wait_recv()
            begin(remote(part, part, ags_sem.at[i, 6 + k], agr_sem.at[i, 6 + k], partner))

    def ag_end(i):
        for k in range(1, tpn):
            sq_ref = (gains if i == 0 else squares).at[lax.rem(tp + tpn - k, tpn)]
            remote(sq_ref, sq_ref, sqs_sem.at[i, k], sqr_sem.at[i, k], partner).wait_recv()
        if i > 0:
            total = squares[0]
            for k in range(1, tpn):
                total = total + squares[k]
            factor = lax.rsqrt(total * (1.0 / features) + EPS)
            for r in range(3):
                factors[r * tile:(r + 1) * tile] = jnp.broadcast_to(factor[r:r + 1], (128, 128)).T
        block = acts.at[i, tp + 1 - 2 * core]
        remote(block, block, ags_sem.at[i, 0], agr_sem.at[i, 0], partner).wait_recv()
        for side in range(3):
            for h in range(2):
                part = ag_part(i, side, h, True)
                k = 7 + 2 * side + h
                remote(part, part, ags_sem.at[i, k], agr_sem.at[i, k], partner).wait_recv()

    def whole(i):
        return jnp.concatenate([acts[i, k] for k in range(tpn)], axis=1)

    def factors_from_sum():
        total = jnp.sum(sq_sum[...], axis=1, keepdims=True)
        factors[...] = jnp.broadcast_to(lax.rsqrt(total * (1.0 / features) + EPS), (rows, 128))

    def scale_input(k):
        wide = acts[0, k].astype(F32)
        acts[1, k] = (wide * gains[k, 0].astype(F32)).astype(BF16)
        sq = wide * wide
        both = sq[:, :128] + sq[:, 128:]
        sq_sum[...] = both if k == 0 else sq_sum[...] + both

    chunk = rows // tpn

    def rows_at(o, c):
        return pl.ds(pl.multiple_of((2 * lax.rem(x + o, RING_X) + c) * chunk, 16), chunk)

    def g_remote(g, src, dst, k, dev):
        return remote(src, dst, gs_sem.at[g, k], gr_sem.at[g, k], dev)

    def g_wait(g, ref, k):
        g_remote(g, ref, ref, k, partner).wait_recv()

    def paired_sum(g, k, h):
        return part[g, h, rows_at(NEAR[k], core)] + gp_in[g, k, h].astype(F32)

    x_dev = (x_right, x_left)

    def g_multiply(g):
        for h in range(2):
            for d in BATCH[g][h]:
                if d != 0:
                    y_wait(1, d)
        for h in range(2):
            d0, d1 = BATCH[g][h]
            parts = []
            for t in range(3):
                for q in range(2):
                    parts.append(jnp.concatenate([wd[t, q, shard(d0)], wd[t, q, shard(d1)]], axis=1))
            part[g, h] = jnp.dot(hidden[...], jnp.concatenate(parts, axis=0), preferred_element_type=F32)
        for k, o in enumerate(NEAR):
            for h in range(2):
                gp_out[g, k, h] = part[g, h, rows_at(o, 1 - core)].astype(BF16)
        begin(g_remote(g, gp_out.at[g], gp_in.at[g], 0, partner))

    def g_pair(g):
        g_wait(g, gp_in.at[g], 0)
        for h in range(2):
            gt_out[g, 0, h] = paired_sum(g, 0, h).astype(BF16)
            begin(g_remote(g, gt_out.at[g, 0, h], gm_in.at[g, h], 1 + h, x_dev[h]))
        for side in range(2):
            gt_out[g, 1 + side, 1 - side] = paired_sum(g, 1 + side, 1 - side).astype(BF16)
            begin(g_remote(
                g, gt_out.at[g, 1 + side, 1 - side], gl_in.at[g, side, 1 - side], 3 + 2 * side + 1 - side, x_dev[side]
            ))

    def g_turn(g):
        for side in range(2):
            g_wait(g, gm_in.at[g, side], 1 + side)
            gt_out[g, 1 + side, side] = (paired_sum(g, 1 + side, side) + gm_in[g, side].astype(F32)).astype(BF16)
            begin(g_remote(g, gt_out.at[g, 1 + side, side], gl_in.at[g, side, side], 3 + 3 * side, x_dev[side]))

    def g_first(g):
        for side in range(2):
            for h in range(2):
                g_wait(g, gl_in.at[g, side, h], 3 + 2 * side + h)
        for h in range(2):
            total = paired_sum(g, 3, h) + gl_in[g, 0, h].astype(F32) + gl_in[g, 1, h].astype(F32)
            for e in range(2):
                b = shard(BATCH[g][h][e])
                both = acts[0, b // 2, pl.ds(pl.multiple_of(tp * chunk, 16), chunk)].astype(F32)
                base = jnp.where(b % 2 == 1, both[:, 128:], both[:, :128])
                cols = slice(e * 128, (e + 1) * 128)
                fall[g, tp, h, :, cols] = (base + 0.5 * total[:, cols]).astype(BF16)
        block = fall.at[g, tp]
        begin(g_remote(g, block, block, 8, x_right))
        begin(g_remote(g, block, block, 9, x_left))
        begin(g_remote(g, block, block, 7, partner))

    def fall_of(g, o, c):
        return fall.at[g, 2 * lax.rem(x + o, RING_X) + c]

    def g_near(g):
        for side in range(2):
            block = fall_of(g, (RING_X - 1, 1)[side], core)
            g_wait(g, block, 8 + side)
            begin(g_remote(g, block.at[side], block.at[side], 10 + side, x_dev[side]))
            begin(g_remote(g, block, block, 12 + side, partner))

    def g_far(g):
        block = fall_of(g, 2, core)
        for h in range(2):
            g_wait(g, block.at[h], 10 + h)
            begin(g_remote(g, block.at[h], block.at[h], 14 + h, partner))

    def g_end(g):
        g_wait(g, fall_of(g, 0, 1 - core), 7)
        g_wait(g, fall_of(g, RING_X - 1, 1 - core), 12)
        g_wait(g, fall_of(g, 1, 1 - core), 13)
        for h in range(2):
            g_wait(g, fall_of(g, 2, 1 - core).at[h], 14 + h)
        for h in range(2):
            for e in range(2):
                b = shard(BATCH[g][h][e])
                value = jnp.concatenate([fall[g, k, h, :, e * 128:(e + 1) * 128] for k in range(tpn)], axis=0)
                first_all[b] = value
                wide = value.astype(F32)
                gain = gains[b // 2, 1].astype(F32)
                gain = jnp.where(b % 2 == 1, gain[:, 128:], gain[:, :128])
                scaled_all[b] = (wide * gain).astype(BF16)
                sq = wide * wide
                sq_sum[...] = sq if g == h == e == 0 else sq_sum[...] + sq
        blocks = [shard(d) for pair in BATCH[g] for d in pair]
        left = jnp.concatenate([scaled_all[b] for b in blocks], axis=1)
        right = jnp.concatenate(
            [jnp.concatenate([wpg[t, rows_of(b)] for t in range(3)], axis=1) for b in blocks], axis=0
        )
        product = jnp.dot(left, right, preferred_element_type=F32)
        mixed_in[...] = product if g == 0 else mixed_in[...] + product

    def rs(i, block):
        def at(o, c):
            return 2 * lax.rem(x + o, RING_X) + c

        for k, o in enumerate(NEAR):
            pair_out[i, k] = block(at(o, 1 - core)).astype(BF16)
            begin(remote(pair_out.at[i, k], pair_in.at[i, k], rss_sem.at[i, k], rsr_sem.at[i, k], partner))

        def paired(k):
            product = block(at(NEAR[k], core))
            remote(pair_out.at[i, k], pair_in.at[i, k], rss_sem.at[i, k], rsr_sem.at[i, k], partner).wait_recv()
            return product + pair_in[i, k].astype(F32)

        low = pl.ds(0, half_rows)
        high = pl.ds(half_rows, half_rows)
        turn_out[i, 0] = paired(0).astype(BF16)
        begin(remote(turn_out.at[i, 0, low], mid_in.at[i, 0], rss_sem.at[i, 4], rsr_sem.at[i, 4], x_right))
        begin(remote(turn_out.at[i, 0, high], mid_in.at[i, 1], rss_sem.at[i, 5], rsr_sem.at[i, 5], x_left))
        right = paired(1)
        turn_out[i, 1, half_rows:] = right[half_rows:].astype(BF16)
        begin(remote(turn_out.at[i, 1, high], last_in.at[i, 0, high], rss_sem.at[i, 7], rsr_sem.at[i, 7], x_right))
        kept[0] = right[:half_rows]
        left = paired(2)
        turn_out[i, 2, :half_rows] = left[:half_rows].astype(BF16)
        begin(remote(turn_out.at[i, 2, low], last_in.at[i, 1, low], rss_sem.at[i, 8], rsr_sem.at[i, 8], x_left))
        kept[1] = left[half_rows:]
        own[...] = paired(3)
        remote(turn_out.at[i, 0, low], mid_in.at[i, 0], rss_sem.at[i, 4], rsr_sem.at[i, 4], x_right).wait_recv()
        turn_out[i, 1, :half_rows] = (kept[0] + mid_in[i, 0].astype(F32)).astype(BF16)
        begin(remote(turn_out.at[i, 1, low], last_in.at[i, 0, low], rss_sem.at[i, 6], rsr_sem.at[i, 6], x_right))
        remote(turn_out.at[i, 0, high], mid_in.at[i, 1], rss_sem.at[i, 5], rsr_sem.at[i, 5], x_left).wait_recv()
        turn_out[i, 2, half_rows:] = (kept[1] + mid_in[i, 1].astype(F32)).astype(BF16)
        begin(remote(turn_out.at[i, 2, high], last_in.at[i, 1, high], rss_sem.at[i, 9], rsr_sem.at[i, 9], x_left))
        for k, side, part in ((7, 0, high), (8, 1, low), (6, 0, low), (9, 1, high)):
            ref = last_in.at[i, side, part]
            remote(ref, ref, rss_sem.at[i, k], rsr_sem.at[i, k], x_right).wait_recv()
        return own[...] + last_in[i, 0].astype(F32) + last_in[i, 1].astype(F32)

    def gu(i, t):
        scaled = whole(i)
        for q in range(2):
            pre[q] = jnp.dot(scaled, wgu[q, t], preferred_element_type=F32)
        for s in range(third // 128):
            cols = slice(s * 128, (s + 1) * 128)
            gate = factors[...] * pre[0, :, cols]
            up = factors[...] * pre[1, :, cols]
            hidden[:, t * third + s * 128:t * third + (s + 1) * 128] = (gate / (1.0 + jnp.exp(-gate)) * up).astype(BF16)

    def down_block(j):
        parts = []
        for t in range(3):
            for h in range(2):
                parts.append(jnp.concatenate([wd[t, h, 2 * j], wd[t, h, 2 * j + 1]], axis=1))
        return jnp.dot(hidden[...], jnp.concatenate(parts, axis=0), preferred_element_type=F32)

    for copy in local[:early]:
        copy.wait()
    head, tail = (0, 1, 2, 3), (4, 5, 6, 7)
    for k in (0, 1):
        for direction in range(2):
            z_send(k, direction, 0)
    ag_begin(0, xin[...])
    for copy in local[early:]:
        copy.wait()
    for k in (2, 3):
        for direction in range(2):
            z_send(k, direction, 0)
    for step in range(1, half_n + 1):
        if step == half_n:
            for k in tail:
                for direction in range(2):
                    z_send(k, direction, 0)
        z_step(head, (0, 2), step)
        if step == 1:
            ag_near(0)
        if step == 2:
            ag_far(0)
        if step == 3:
            ag_end(0)
        if 4 <= step < 8:
            scale_input(2 * step - 8)
            scale_input(2 * step - 7)
    factors_from_sum()
    stages = (g_multiply, g_pair, g_turn, g_first, g_near, g_far, g_end)
    for slot in range(1, 2 * half_n):
        if slot <= half_n:
            z_step(tail, (1,), slot)
        if slot == 2:
            y_wait_all(0)
            gu(1, 0)
            gu(1, 1)
        if slot == 3:
            gu(1, 2)
        if slot == half_n:
            y_wait_all(2)
        for k, stage in reversed(tuple(enumerate(stages))):
            g = (slot - 3 - k) // 2
            if (slot - 3 - k) % 2 == 0 and 0 <= g < len(BATCH):
                stage(g)
    factors_from_sum()
    first[...] = jnp.concatenate([first_all[2 * tp], first_all[2 * tp + 1]], axis=1)

    pool_pre = (factors[...] * mixed_in[:, :128]).astype(BF16)
    for s in range(2):
        logit = factors[...] * mixed_in[:, (1 + s) * 128:(2 + s) * 128]
        pre[0, :, s * 128:(s + 1) * 128] = 1.0 / (1.0 + jnp.exp(-logit))
    values = pool_pre.astype(F32)
    position = lax.broadcasted_iota(jnp.int32, (rows, 128), 0)
    window_id = lax.rem(tp, 4)
    running = values
    chosen = values
    for w in range(4):
        span = 1 << w
        lagged = jnp.where(position >= span, pltpu.roll(running, span, 0), 0.0)
        running = running + lagged
        counts = jnp.minimum(position + 1, 2 * span).astype(F32)
        chosen = jnp.where(window_id == w, running / counts, chosen)
    trail = (chosen - values).astype(BF16)
    mixed = jnp.dot(trail, mixw[0], preferred_element_type=F32)
    hidden[:, :128] = (mixed * pscale[...]).astype(BF16)

    def lift_block(j):
        both = jnp.concatenate([wo[2 * j], wo[2 * j + 1]], axis=1)
        return jnp.dot(hidden[:, :128], both, preferred_element_type=F32)

    total = rs(1, lift_block)
    second[...] = (first[...].astype(F32) + pre[0] * total).astype(BF16)
    ag_begin(2, second[...])
    ag_near(2)
    ag_far(2)
    ag_end(2)
    for t in range(3):
        gu(2, t)
    total = rs(2, down_block)
    out_ref[...] = (second[...].astype(F32) + 0.5 * total).astype(BF16)
    for copy in sent:
        copy.wait_send()


def per_device(n, tpn, *arrays):
    x, gate = arrays[0], arrays[2]
    rows, width = x.shape
    kdim, ff = gate.shape
    third = ff // 3
    chunk = rows // tpn
    vmem = pltpu.VMEM
    dma = pltpu.SemaphoreType.DMA
    half_n = n // 2
    any_spec = pl.BlockSpec(memory_space=pl.ANY)
    return pl.pallas_call(
        functools.partial(kernel, n),
        out_shape=jax.ShapeDtypeStruct((rows, width), BF16),
        in_specs=[any_spec] * len(arrays),
        out_specs=pl.BlockSpec(memory_space=pltpu.VMEM),
        scratch_shapes=[
            vmem((rows, width), BF16),
            vmem((tpn, 3, 1, width), BF16),
            vmem((1, 128, 128), BF16),
            vmem((1, 128), F32),
            vmem((2, 3, n * kdim, third), BF16),
            vmem((3, 2, n, third // 2, 128), BF16),
            vmem((3, n * kdim, 128), BF16),
            vmem((n, 128, 128), BF16),
            vmem((3, tpn, rows, width), BF16),
            vmem((tpn, 8, 128), F32),
            vmem((rows, 128), F32),
            vmem((rows, ff), BF16),
            vmem((2, rows, third), F32),
            vmem((rows, width), BF16),
            vmem((rows, width), BF16),
            vmem((rows, 384), F32),
            vmem((4, 2, rows, width), F32),
            vmem((4, 4, 2, chunk, width), BF16),
            vmem((4, 4, 2, chunk, width), BF16),
            vmem((4, 3, 2, chunk, width), BF16),
            vmem((4, 2, chunk, width), BF16),
            vmem((4, 2, 2, chunk, width), BF16),
            vmem((4, tpn, 2, chunk, width), BF16),
            vmem((n, rows, 128), BF16),
            vmem((n, rows, 128), BF16),
            vmem((rows, 128), F32),
            vmem((3, 4, rows, width), BF16),
            vmem((3, 4, rows, width), BF16),
            vmem((3, 3, rows, width), BF16),
            vmem((3, 2, rows // 2, width), BF16),
            vmem((3, 2, rows, width), BF16),
            vmem((2, rows // 2, width), F32),
            vmem((rows, width), F32),
            dma((24,)),
            dma((8, 2, half_n)),
            dma((8, 2, half_n)),
            dma((3, n)),
            dma((3, n)),
            dma((3, 13)),
            dma((3, 13)),
            dma((3, tpn)),
            dma((3, tpn)),
            dma((3, 10)),
            dma((3, 10)),
            dma((4, 16)),
            dma((4, 16)),
        ],
        compiler_params=pltpu.CompilerParams(
            collective_id=0, has_side_effects=True, vmem_limit_bytes=60 * 1024 * 1024
        ),
    )(*arrays)


def solution(mesh):
    return jax.shard_map(
        functools.partial(per_device, mesh.shape["fs"], mesh.shape["tp"]),
        mesh=mesh,
        in_specs=(
            P(("grp", "fs"), "tp"),
            P(None, "tp"),
            P("fs", "tp"),
            P("fs", "tp"),
            P("tp", "fs"),
            P(None, "tp"),
            P("fs", "tp"),
            P("fs", "tp"),
            P("tp", None, None),
            P(None, "tp"),
            P("tp", "fs"),
            P(None, "tp"),
        ),
        out_specs=P(("grp", "fs"), "tp"),
        check_vma=False,
    )
```

```python
import functools

import jax
import jax.numpy as jnp
from jax import lax
from jax.experimental import pallas as pl
from jax.experimental.pallas import tpu as pltpu
from jax.sharding import PartitionSpec as P

F32 = jnp.float32
BF16 = jnp.bfloat16
MESH = pl.DeviceIdType.MESH
EPS = 1e-06
RING_X = 4
NEAR = (2, 1, 3, 0)


def remote(src, dst, send, recv, device):
    return pltpu.make_async_remote_copy(
        src_ref=src, dst_ref=dst, send_sem=send, recv_sem=recv, device_id=device, device_id_type=MESH
    )


def kernel(
    n,
    x_hbm, g1_hbm, gate_hbm, up_hbm, down_hbm, gm_hbm, pin_hbm, mg_hbm, mix_hbm, ps_hbm, mo_hbm, g2_hbm,
    out_ref,
    xin, gains, mixw, pscale,
    wgu, wd, wpg, wo,
    acts, squares, factors, hidden, pre, opened, pooling, first, second,
    pair_out, pair_in, turn_out, mid_in, last_in, kept, own,
    in_sem,
    zs_sem, zr_sem, ys_sem, yr_sem,
    ags_sem, agr_sem, sqs_sem, sqr_sem, rss_sem, rsr_sem,
):
    rows, width = x_hbm.shape
    part_rows = rows // 2
    half_rows = part_rows // 2
    kdim = gate_hbm.shape[0]
    third = gate_hbm.shape[1] // 3
    half_third = third // 2
    tpn = lax.axis_size("tp")
    features = tpn * width

    grp = lax.axis_index("grp")
    fs = lax.axis_index("fs")
    tp = lax.axis_index("tp")
    x = tp // 2
    core = tp % 2
    parity = grp % 2
    mine = 2 * parity
    other = 2 - mine

    z_right = {"fs": lax.rem(fs + 1, n)}
    z_left = {"fs": lax.rem(fs + n - 1, n)}
    z_dev = (z_right, z_left)
    y_dev = {"grp": grp + 1 - 2 * parity}
    partner = {"tp": tp + 1 - 2 * core}
    x_right = {"tp": lax.rem(tp + 2, tpn)}
    x_left = {"tp": lax.rem(tp + tpn - 2, tpn)}

    sent = []

    def begin(copy):
        copy.start()
        sent.append(copy)

    own_rows = pl.ds(pl.multiple_of(fs * kdim, kdim), kdim)
    local = []

    def fetch(src, dst):
        copy = pltpu.make_async_copy(src, dst, in_sem.at[len(local)])
        copy.start()
        local.append(copy)

    for q, ref in enumerate((gate_hbm, up_hbm)):
        for t in range(3):
            fetch(ref.at[:, pl.ds(t * third, third)], wgu.at[q, t, own_rows])
    fetch(x_hbm, xin)
    for k, ref in enumerate((g1_hbm, gm_hbm, g2_hbm)):
        fetch(ref, gains.at[k])
    early = len(local)
    for t in range(3):
        for h in range(2):
            fetch(down_hbm.at[pl.ds(t * third + h * half_third, half_third)], wd.at[t, h, fs])
    fetch(pin_hbm, wpg.at[0, own_rows])
    for t in range(2):
        fetch(mg_hbm.at[:, pl.ds(t * 128, 128)], wpg.at[1 + t, own_rows])
    fetch(mo_hbm, wo.at[fs])
    fetch(mix_hbm, mixw)
    fetch(ps_hbm, pscale)

    barrier = pltpu.get_barrier_semaphore()
    for dev in (z_right, z_left, y_dev):
        pl.semaphore_signal(barrier, inc=1, device_id=dev, device_id_type=MESH)
    for k in range(1, tpn):
        pl.semaphore_signal(barrier, inc=1, device_id={"tp": lax.rem(tp + k, tpn)}, device_id_type=MESH)
    pl.semaphore_wait(barrier, 3 + tpn - 1)

    def shard(d):
        return lax.rem(fs + n + d, n)

    def rows_of(s):
        return pl.ds(pl.multiple_of(s * kdim, kdim), kdim)

    def z_gu(q):
        return lambda s: wgu.at[q, pl.ds(parity, 2), rows_of(s)]

    def z_down(slot, q):
        return lambda s: wd.at[slot, q, s]

    def z_pool(t):
        return lambda s: wpg.at[t, rows_of(s)]

    half_n = n // 2
    gu_ks, down_ks, mix_ks = (0, 1), (2, 3, 4, 5), (6, 7, 8, 9)
    chains = (
        z_gu(0), z_gu(1), z_down(mine, 0), z_down(mine, 1), z_down(1, 0), z_down(1, 1),
        z_pool(0), z_pool(1), z_pool(2), lambda s: wo.at[s],
    )
    hops = ((half_n, half_n - 1), (half_n - 1, half_n)) * 5

    def y_gu(q):
        return lambda slot, s: wgu.at[q, slot, rows_of(s)]

    def y_down(slot, s):
        return wd.at[slot, :, s]

    y_kinds = (y_gu(0), y_gu(1), y_down)

    def z_send(k, direction, step):
        region = chains[k](shard(-step if direction == 0 else step))
        begin(remote(region, region, zs_sem.at[k, direction, step], zr_sem.at[k, direction, step], z_dev[direction]))

    def z_wait(k, direction, step):
        region = chains[k](shard(-step if direction == 0 else step))
        remote(
            region, region, zs_sem.at[k, direction, step - 1], zr_sem.at[k, direction, step - 1], z_dev[direction]
        ).wait_recv()
        if step < hops[k][direction]:
            z_send(k, direction, step)

    def y_send(kind, d):
        region = y_kinds[kind](mine, shard(d))
        begin(remote(region, region, ys_sem.at[kind, d % n], yr_sem.at[kind, d % n], y_dev))

    def y_wait_all(kind):
        for step in range(1, half_n + 1):
            for d in (-step, step) if step < half_n else (step,):
                region = y_kinds[kind](other, shard(d))
                remote(region, region, ys_sem.at[kind, d % n], yr_sem.at[kind, d % n], y_dev).wait_recv()

    def z_step(ks, step):
        for k in ks:
            for direction in range(2):
                if step <= hops[k][direction]:
                    z_wait(k, direction, step)
                    if k in gu_ks:
                        y_send(k, -step if direction == 0 and step < half_n else step)
            if k == down_ks[1]:
                for d in (-step, step) if step < half_n else (step,):
                    y_send(2, d)

    def ag_part(i, u, side, h, other_core=False):
        offset = (RING_X - 1, 1, 2)[side]
        c = 1 - core if other_core else core
        return acts.at[i, u, 2 * lax.rem(x + offset, RING_X) + c, pl.ds(h * half_rows, half_rows)]

    def ag(i, u, values):
        def move(ref, k, dev):
            return remote(ref, ref, ags_sem.at[i, u, k], agr_sem.at[i, u, k], dev)

        def move_sq(ref, k, dev):
            return remote(ref, ref, sqs_sem.at[i, u, k], sqr_sem.at[i, u, k], dev)

        wide = values.astype(F32)
        acts[i, u, tp] = (wide * gains[i].astype(F32)).astype(BF16)
        block = acts.at[i, u, tp]
        for h, dev, base in ((0, x_right, 1), (1, x_left, 3), (1, x_right, 1), (0, x_left, 3)):
            begin(move(block.at[pl.ds(h * half_rows, half_rows)], base + h, dev))
        begin(move(block, 0, partner))
        sq = wide * wide
        folded = sq[:, :128] + sq[:, 128:]
        squares[i, u, tp] = jnp.zeros((8, 128), F32)
        for r in range(2):
            start = r * (part_rows - 128)
            squares[i, u, tp, r:r + 1] = jnp.sum(folded[start:start + 128].T, axis=0, keepdims=True)
        for k in range(1, tpn):
            begin(move_sq(squares.at[i, u, tp], k, {"tp": lax.rem(tp + k, tpn)}))
        yield
        for side, h in ((0, 0), (1, 1), (0, 1), (1, 0)):
            part = ag_part(i, u, side, h)
            k = 1 + 2 * side + h
            move(part, k, partner).wait_recv()
            if side == h:
                begin(move(part, 5 + h, (x_right, x_left)[side]))
            begin(move(part, 6 + k, partner))
        yield
        for h in range(2):
            part = ag_part(i, u, 2, h)
            move(part, 5 + h, partner).wait_recv()
            begin(move(part, 11 + h, partner))
        yield
        for k in range(1, tpn):
            move_sq(squares.at[i, u, lax.rem(tp + tpn - k, tpn)], k, partner).wait_recv()
        total = squares[i, u, 0]
        for k in range(1, tpn):
            total = total + squares[i, u, k]
        factor = lax.rsqrt(total * (1.0 / features) + EPS)
        tall = [jnp.broadcast_to(factor[r:r + 1], (128, 128)).T for r in range(2)]
        factors[i, u, :128] = tall[0]
        factors[i, u, 128:] = tall[1][256 - part_rows:]
        move(acts.at[i, u, tp + 1 - 2 * core], 0, partner).wait_recv()
        for side in range(3):
            for h in range(2):
                move(ag_part(i, u, side, h, True), 7 + 2 * side + h, partner).wait_recv()

    def whole(i, u):
        return jnp.concatenate([acts[i, u, k] for k in range(tpn)], axis=1)

    def half(u):
        return slice(u * part_rows, (u + 1) * part_rows)

    def rs(i, u, block, finish):
        def at(o, c):
            return 2 * lax.rem(x + o, RING_X) + c

        def move(src, dst, k, dev):
            return remote(src, dst, rss_sem.at[i, u, k], rsr_sem.at[i, u, k], dev)

        out, turn, kept_u = pair_out.at[i, u], turn_out.at[i, u], kept.at[u]
        came, mid, last = pair_in.at[i, u], mid_in.at[i, u], last_in.at[i, u]
        for k, o in enumerate(NEAR):
            out[k] = block(at(o, 1 - core)).astype(BF16)
            begin(move(out.at[k], came.at[k], k, partner))
        yield

        def paired(k):
            product = block(at(NEAR[k], core))
            move(out.at[k], came.at[k], k, partner).wait_recv()
            return product + came[k].astype(F32)

        low = pl.ds(0, half_rows)
        high = pl.ds(half_rows, half_rows)
        turn[0] = paired(0).astype(BF16)
        begin(move(turn.at[0, low], mid.at[0], 4, x_right))
        begin(move(turn.at[0, high], mid.at[1], 5, x_left))
        right = paired(1)
        turn[1, half_rows:] = right[half_rows:].astype(BF16)
        begin(move(turn.at[1, high], last.at[0, high], 7, x_right))
        kept_u[0] = right[:half_rows]
        left = paired(2)
        turn[2, :half_rows] = left[:half_rows].astype(BF16)
        begin(move(turn.at[2, low], last.at[1, low], 8, x_left))
        kept_u[1] = left[half_rows:]
        own[u] = paired(3)
        yield
        move(mid.at[0], mid.at[0], 4, x_right).wait_recv()
        turn[1, :half_rows] = (kept_u[0] + mid[0].astype(F32)).astype(BF16)
        begin(move(turn.at[1, low], last.at[0, low], 6, x_right))
        move(mid.at[1], mid.at[1], 5, x_left).wait_recv()
        turn[2, half_rows:] = (kept_u[1] + mid[1].astype(F32)).astype(BF16)
        begin(move(turn.at[2, high], last.at[1, high], 9, x_left))
        yield
        for k, side, part in ((7, 0, high), (8, 1, low), (6, 0, low), (9, 1, high)):
            move(last.at[side, part], last.at[side, part], k, x_right).wait_recv()
        finish(own[u] + last[0].astype(F32) + last[1].astype(F32))

    def gu(i, u, t):
        scaled = whole(i, u)
        for q in range(2):
            pre[q] = jnp.dot(scaled, wgu[q, t], preferred_element_type=F32)
        for s in range(third // 128):
            cols = slice(s * 128, (s + 1) * 128)
            gate = factors[i, u] * pre[0, :, cols]
            up = factors[i, u] * pre[1, :, cols]
            hidden[half(u), t * third + s * 128:t * third + (s + 1) * 128] = (
                gate / (1.0 + jnp.exp(-gate)) * up
            ).astype(BF16)

    def down_block(u):
        def block(j):
            parts = []
            for t in range(3):
                for h in range(2):
                    parts.append(jnp.concatenate([wd[t, h, 2 * j], wd[t, h, 2 * j + 1]], axis=1))
            return jnp.dot(hidden[half(u)], jnp.concatenate(parts, axis=0), preferred_element_type=F32)

        return block

    def lift_block(u):
        def block(j):
            both = jnp.concatenate([wo[2 * j], wo[2 * j + 1]], axis=1)
            return jnp.dot(hidden[half(u), :128], both, preferred_element_type=F32)

        return block

    def set_first(u):
        def finish(total):
            first[half(u)] = (xin[half(u)].astype(F32) + 0.5 * total).astype(BF16)

        return finish

    def set_second(u):
        def finish(total):
            second[half(u)] = (first[half(u)].astype(F32) + opened[half(u)] * total).astype(BF16)

        return finish

    def set_out(u):
        def finish(total):
            out_ref[half(u)] = (second[half(u)].astype(F32) + 0.5 * total).astype(BF16)

        return finish

    def mix(u):
        weights = jnp.concatenate([wpg[t] for t in range(3)], axis=1)
        sums = jnp.dot(whole(1, u), weights, preferred_element_type=F32)
        scale = factors[1, u]
        for s in range(2):
            logit = scale * sums[:, (1 + s) * 128:(2 + s) * 128]
            opened[half(u), s * 128:(s + 1) * 128] = 1.0 / (1.0 + jnp.exp(-logit))
        pooling[16 + u * part_rows:16 + (u + 1) * part_rows] = (scale * sums[:, :128]).astype(BF16).astype(F32)
        if u == 0:
            pooling[:16] = jnp.zeros((16, 128), F32)
        size = part_rows + 16
        values = pooling[u * part_rows:u * part_rows + size]
        position = lax.broadcasted_iota(jnp.int32, (size, 128), 0) + (u * part_rows - 16)
        window_id = lax.rem(tp, 4)
        running = values
        chosen = values
        for w in range(4):
            span = 1 << w
            running = running + pltpu.roll(running, span, 0)
            counts = jnp.clip(position + 1, 1, 2 * span).astype(F32)
            chosen = jnp.where(window_id == w, running / counts, chosen)
        trail = (chosen - values)[16:].astype(BF16)
        mixed = jnp.dot(trail, mixw[0], preferred_element_type=F32)
        hidden[half(u), :128] = (mixed * pscale[...]).astype(BF16)

    def layer(u):
        yield from rs(0, u, down_block(u), set_first(u))
        yield from ag(1, u, first[half(u)])
        mix(u)
        yield from rs(1, u, lift_block(u), set_second(u))
        yield from ag(2, u, second[half(u)])
        for t in range(3):
            gu(2, u, t)
        yield from rs(2, u, down_block(u), set_out(u))

    def advance(steps):
        for step in steps:
            next(step, None)

    def send_own(ks):
        for k in ks:
            for direction in range(2):
                z_send(k, direction, 0)

    for copy in local[:early]:
        copy.wait()
    send_own(gu_ks)
    inputs = [ag(0, u, xin[half(u)]) for u in range(2)]
    advance(inputs)
    for copy in local[early:]:
        copy.wait()
    for step in range(1, half_n + 1):
        if step == half_n:
            send_own(down_ks)
        z_step(gu_ks, step)
        if step > 1:
            advance(inputs)
    todo = [(u, t) for u in range(2) for t in range(3)]
    for step in range(1, half_n + 1):
        if step == half_n - 1:
            send_own(mix_ks)
        z_step(down_ks, step)
        if step == 2:
            y_wait_all(0)
            y_wait_all(1)
        if step >= 2:
            for u, t in todo[:2 if step in (3, 4) else 1]:
                gu(0, u, t)
            todo = todo[2 if step in (3, 4) else 1:]
    mix_steps = list(range(1, half_n + 1))

    def mix_step():
        if mix_steps:
            z_step(mix_ks, mix_steps.pop(0))

    mix_step()
    y_wait_all(2)
    mix_step()
    halves = [layer(u) for u in range(2)]
    for turn_number in range(24):
        advance(halves)
        mix_step()
    for copy in sent:
        copy.wait_send()


def per_device(n, tpn, *arrays):
    x, gate = arrays[0], arrays[2]
    rows, width = x.shape
    kdim, ff = gate.shape
    third = ff // 3
    part = rows // 2
    vmem = pltpu.VMEM
    dma = pltpu.SemaphoreType.DMA
    half_n = n // 2
    any_spec = pl.BlockSpec(memory_space=pl.ANY)
    return pl.pallas_call(
        functools.partial(kernel, n),
        out_shape=jax.ShapeDtypeStruct((rows, width), BF16),
        in_specs=[any_spec] * len(arrays),
        out_specs=pl.BlockSpec(memory_space=pltpu.VMEM),
        scratch_shapes=[
            vmem((rows, width), BF16),
            vmem((3, 1, width), BF16),
            vmem((1, 128, 128), BF16),
            vmem((1, 128), F32),
            vmem((2, 3, n * kdim, third), BF16),
            vmem((3, 2, n, third // 2, 128), BF16),
            vmem((3, n * kdim, 128), BF16),
            vmem((n, 128, 128), BF16),
            vmem((3, 2, tpn, part, width), BF16),
            vmem((3, 2, tpn, 8, 128), F32),
            vmem((3, 2, part, 128), F32),
            vmem((rows, ff), BF16),
            vmem((2, part, third), F32),
            vmem((rows, width), F32),
            vmem((rows + 16, 128), F32),
            vmem((rows, width), BF16),
            vmem((rows, width), BF16),
            vmem((3, 2, 4, part, width), BF16),
            vmem((3, 2, 4, part, width), BF16),
            vmem((3, 2, 3, part, width), BF16),
            vmem((3, 2, 2, part // 2, width), BF16),
            vmem((3, 2, 2, part, width), BF16),
            vmem((2, 2, part // 2, width), F32),
            vmem((2, part, width), F32),
            dma((24,)),
            dma((10, 2, half_n)),
            dma((10, 2, half_n)),
            dma((3, n)),
            dma((3, n)),
            dma((3, 2, 13)),
            dma((3, 2, 13)),
            dma((3, 2, tpn)),
            dma((3, 2, tpn)),
            dma((3, 2, 10)),
            dma((3, 2, 10)),
        ],
        compiler_params=pltpu.CompilerParams(
            collective_id=0, has_side_effects=True, vmem_limit_bytes=60 * 1024 * 1024
        ),
    )(*arrays)


def solution(mesh):
    return jax.shard_map(
        functools.partial(per_device, mesh.shape["fs"], mesh.shape["tp"]),
        mesh=mesh,
        in_specs=(
            P(("grp", "fs"), "tp"),
            P(None, "tp"),
            P("fs", "tp"),
            P("fs", "tp"),
            P("tp", "fs"),
            P(None, "tp"),
            P("fs", "tp"),
            P("fs", "tp"),
            P("tp", None, None),
            P(None, "tp"),
            P("tp", "fs"),
            P(None, "tp"),
        ),
        out_specs=P(("grp", "fs"), "tp"),
        check_vma=False,
    )
```

```python
import functools

import jax
import jax.numpy as jnp
from jax import lax
from jax.experimental import pallas as pl
from jax.experimental.pallas import tpu as pltpu
from jax.sharding import PartitionSpec as P

F32 = jnp.float32
BF16 = jnp.bfloat16
MESH = pl.DeviceIdType.MESH
EPS = 1e-06
RING_X = 4
NEAR = (2, 1, 3, 0)


def remote(src, dst, send, recv, device):
    return pltpu.make_async_remote_copy(
        src_ref=src, dst_ref=dst, send_sem=send, recv_sem=recv, device_id=device, device_id_type=MESH
    )


def kernel(
    n,
    x_hbm, g1_hbm, gate_hbm, up_hbm, down_hbm, gm_hbm, pin_hbm, mg_hbm, mix_hbm, ps_hbm, mo_hbm, g2_hbm,
    out_ref,
    xin, gains, mixw, pscale,
    wgu, wd, wpg, wo,
    acts, squares, core_sums, factors, hidden, pre, opened, pooling, first, second,
    pair_out, pair_in, turn_out, mid_in, last_in, kept, own,
    in_sem,
    zs_sem, zr_sem, ys_sem, yr_sem,
    ags_sem, agr_sem, sqs_sem, sqr_sem, rss_sem, rsr_sem,
):
    rows, width = x_hbm.shape
    part_rows = rows // 2
    half_rows = part_rows // 2
    kdim = gate_hbm.shape[0]
    third = gate_hbm.shape[1] // 3
    half_third = third // 2
    tpn = lax.axis_size("tp")
    features = tpn * width

    grp = lax.axis_index("grp")
    fs = lax.axis_index("fs")
    tp = lax.axis_index("tp")
    x = tp // 2
    core = tp % 2
    parity = grp % 2
    mine = 2 * parity
    other = 2 - mine

    z_right = {"fs": lax.rem(fs + 1, n)}
    z_left = {"fs": lax.rem(fs + n - 1, n)}
    z_dev = (z_right, z_left)
    y_dev = {"grp": grp + 1 - 2 * parity}
    partner = {"tp": tp + 1 - 2 * core}
    x_right = {"tp": lax.rem(tp + 2, tpn)}
    x_left = {"tp": lax.rem(tp + tpn - 2, tpn)}

    sent = []

    def begin(copy):
        copy.start()
        sent.append(copy)

    own_rows = pl.ds(pl.multiple_of(fs * kdim, kdim), kdim)
    local = []

    def fetch(src, dst):
        copy = pltpu.make_async_copy(src, dst, in_sem.at[len(local)])
        copy.start()
        local.append(copy)

    for q, ref in enumerate((gate_hbm, up_hbm)):
        for t in range(3):
            fetch(ref.at[:, pl.ds(t * third, third)], wgu.at[q, t, own_rows])
    fetch(x_hbm, xin)
    for k, ref in enumerate((g1_hbm, gm_hbm, g2_hbm)):
        fetch(ref, gains.at[k])
    early = len(local)
    for t in range(3):
        for h in range(2):
            fetch(down_hbm.at[pl.ds(t * third + h * half_third, half_third)], wd.at[t, h, fs])
    fetch(pin_hbm, wpg.at[0, own_rows])
    for t in range(2):
        fetch(mg_hbm.at[:, pl.ds(t * 128, 128)], wpg.at[1 + t, own_rows])
    fetch(mo_hbm, wo.at[fs])
    fetch(mix_hbm, mixw)
    fetch(ps_hbm, pscale)

    barrier = pltpu.get_barrier_semaphore()
    for dev in (z_right, z_left, y_dev):
        pl.semaphore_signal(barrier, inc=1, device_id=dev, device_id_type=MESH)
    for k in range(1, tpn):
        pl.semaphore_signal(barrier, inc=1, device_id={"tp": lax.rem(tp + k, tpn)}, device_id_type=MESH)
    pl.semaphore_wait(barrier, 3 + tpn - 1)

    def shard(d):
        return lax.rem(fs + n + d, n)

    def rows_of(s):
        return pl.ds(pl.multiple_of(s * kdim, kdim), kdim)

    def z_gu(q):
        return lambda s: wgu.at[q, pl.ds(parity, 2), rows_of(s)]

    def z_down(slot, q):
        return lambda s: wd.at[slot, q, s]

    def z_pool(t):
        return lambda s: wpg.at[t, rows_of(s)]

    half_n = n // 2
    gu_ks, down_ks, mix_ks = (0, 1), (2, 3, 4, 5), (6, 7, 8, 9)
    chains = (
        z_gu(0), z_gu(1), z_down(mine, 0), z_down(mine, 1), z_down(1, 0), z_down(1, 1),
        z_pool(0), z_pool(1), z_pool(2), lambda s: wo.at[s],
    )
    hops = ((half_n, half_n - 1), (half_n - 1, half_n)) * 5

    def y_gu(q):
        return lambda slot, s: wgu.at[q, slot, rows_of(s)]

    def y_down(slot, s):
        return wd.at[slot, :, s]

    y_kinds = (y_gu(0), y_gu(1), y_down)

    def z_send(k, direction, step):
        region = chains[k](shard(-step if direction == 0 else step))
        begin(remote(region, region, zs_sem.at[k, direction, step], zr_sem.at[k, direction, step], z_dev[direction]))

    def z_wait(k, direction, step):
        region = chains[k](shard(-step if direction == 0 else step))
        remote(
            region, region, zs_sem.at[k, direction, step - 1], zr_sem.at[k, direction, step - 1], z_dev[direction]
        ).wait_recv()
        if step < hops[k][direction]:
            z_send(k, direction, step)

    def y_send(kind, d):
        region = y_kinds[kind](mine, shard(d))
        begin(remote(region, region, ys_sem.at[kind, d % n], yr_sem.at[kind, d % n], y_dev))

    def y_wait_all(kind):
        for step in range(1, half_n + 1):
            for d in (-step, step) if step < half_n else (step,):
                region = y_kinds[kind](other, shard(d))
                remote(region, region, ys_sem.at[kind, d % n], yr_sem.at[kind, d % n], y_dev).wait_recv()

    def z_step(ks, step):
        for k in ks:
            for direction in range(2):
                if step <= hops[k][direction]:
                    z_wait(k, direction, step)
                    if k in gu_ks:
                        y_send(k, -step if direction == 0 and step < half_n else step)
            if k == down_ks[1]:
                for d in (-step, step) if step < half_n else (step,):
                    y_send(2, d)

    def ag_part(i, u, side, h, other_core=False):
        offset = (RING_X - 1, 1, 2)[side]
        c = 1 - core if other_core else core
        return acts.at[i, u, 2 * lax.rem(x + offset, RING_X) + c, pl.ds(h * half_rows, half_rows)]

    def ag(i, u, values):
        def move(ref, k, dev):
            return remote(ref, ref, ags_sem.at[i, u, k], agr_sem.at[i, u, k], dev)

        def move_sq(ref, k, dev):
            return remote(ref, ref, sqs_sem.at[i, u, k], sqr_sem.at[i, u, k], dev)

        wide = values.astype(F32)
        acts[i, u, tp] = (wide * gains[i].astype(F32)).astype(BF16)
        block = acts.at[i, u, tp]
        for h, dev, base in ((0, x_right, 1), (1, x_left, 3), (1, x_right, 1), (0, x_left, 3)):
            begin(move(block.at[pl.ds(h * half_rows, half_rows)], base + h, dev))
        begin(move(block, 0, partner))
        sq = wide * wide
        folded = sq[:, :128] + sq[:, 128:]
        squares[i, u, tp] = jnp.zeros((8, 128), F32)
        for r in range(2):
            start = r * (part_rows - 128)
            squares[i, u, tp, r:r + 1] = jnp.sum(folded[start:start + 128].T, axis=0, keepdims=True)
        for k in range(2, tpn, 2):
            begin(move_sq(squares.at[i, u, tp], k, {"tp": lax.rem(tp + k, tpn)}))
        yield
        for side, h in ((0, 0), (1, 1), (0, 1), (1, 0)):
            part = ag_part(i, u, side, h)
            k = 1 + 2 * side + h
            move(part, k, partner).wait_recv()
            if side == h:
                begin(move(part, 5 + h, (x_right, x_left)[side]))
            begin(move(part, 6 + k, partner))
        yield
        for h in range(2):
            part = ag_part(i, u, 2, h)
            move(part, 5 + h, partner).wait_recv()
            begin(move(part, 11 + h, partner))
        total = squares[i, u, tp]
        for k in range(2, tpn, 2):
            there = lax.rem(tp + tpn - k, tpn)
            move_sq(squares.at[i, u, there], k, partner).wait_recv()
            total = total + squares[i, u, there]
        core_sums[i, u, 0] = total
        to_other = remote(
            core_sums.at[i, u, 0], core_sums.at[i, u, 1], sqs_sem.at[i, u, 1], sqr_sem.at[i, u, 1], partner
        )
        begin(to_other)
        yield
        to_other.wait_recv()
        total = core_sums[i, u, 0] + core_sums[i, u, 1]
        factor = lax.rsqrt(total * (1.0 / features) + EPS)
        tall = [jnp.broadcast_to(factor[r:r + 1], (128, 128)).T for r in range(2)]
        factors[i, u, :128] = tall[0]
        factors[i, u, 128:] = tall[1][256 - part_rows:]
        move(acts.at[i, u, tp + 1 - 2 * core], 0, partner).wait_recv()
        for side in range(3):
            for h in range(2):
                move(ag_part(i, u, side, h, True), 7 + 2 * side + h, partner).wait_recv()

    def whole(i, u):
        return jnp.concatenate([acts[i, u, k] for k in range(tpn)], axis=1)

    def half(u):
        return slice(u * part_rows, (u + 1) * part_rows)

    def rs(i, u, block, finish):
        def at(o, c):
            return 2 * lax.rem(x + o, RING_X) + c

        def move(src, dst, k, dev):
            return remote(src, dst, rss_sem.at[i, u, k], rsr_sem.at[i, u, k], dev)

        out, turn, kept_u = pair_out.at[i, u], turn_out.at[i, u], kept.at[u]
        came, mid, last = pair_in.at[i, u], mid_in.at[i, u], last_in.at[i, u]
        for k, o in enumerate(NEAR):
            out[k] = block(at(o, 1 - core)).astype(BF16)
            begin(move(out.at[k], came.at[k], k, partner))
        yield

        def paired(k):
            product = block(at(NEAR[k], core))
            move(out.at[k], came.at[k], k, partner).wait_recv()
            return product + came[k].astype(F32)

        low = pl.ds(0, half_rows)
        high = pl.ds(half_rows, half_rows)
        turn[0] = paired(0).astype(BF16)
        begin(move(turn.at[0, low], mid.at[0], 4, x_right))
        begin(move(turn.at[0, high], mid.at[1], 5, x_left))
        right = paired(1)
        turn[1, half_rows:] = right[half_rows:].astype(BF16)
        begin(move(turn.at[1, high], last.at[0, high], 7, x_right))
        kept_u[0] = right[:half_rows]
        left = paired(2)
        turn[2, :half_rows] = left[:half_rows].astype(BF16)
        begin(move(turn.at[2, low], last.at[1, low], 8, x_left))
        kept_u[1] = left[half_rows:]
        own[u] = paired(3)
        yield
        move(mid.at[0], mid.at[0], 4, x_right).wait_recv()
        turn[1, :half_rows] = (kept_u[0] + mid[0].astype(F32)).astype(BF16)
        begin(move(turn.at[1, low], last.at[0, low], 6, x_right))
        move(mid.at[1], mid.at[1], 5, x_left).wait_recv()
        turn[2, half_rows:] = (kept_u[1] + mid[1].astype(F32)).astype(BF16)
        begin(move(turn.at[2, high], last.at[1, high], 9, x_left))
        yield
        for k, side, part in ((7, 0, high), (8, 1, low), (6, 0, low), (9, 1, high)):
            move(last.at[side, part], last.at[side, part], k, x_right).wait_recv()
        finish(own[u] + last[0].astype(F32) + last[1].astype(F32))

    def gu(i, u, t):
        scaled = whole(i, u)
        for q in range(2):
            pre[q] = jnp.dot(scaled, wgu[q, t], preferred_element_type=F32)
        for s in range(third // 128):
            cols = slice(s * 128, (s + 1) * 128)
            gate = factors[i, u] * pre[0, :, cols]
            up = factors[i, u] * pre[1, :, cols]
            hidden[half(u), t * third + s * 128:t * third + (s + 1) * 128] = (
                gate / (1.0 + jnp.exp(-gate)) * up
            ).astype(BF16)

    def down_block(u):
        def block(j):
            parts = []
            for t in range(3):
                for h in range(2):
                    parts.append(jnp.concatenate([wd[t, h, 2 * j], wd[t, h, 2 * j + 1]], axis=1))
            return jnp.dot(hidden[half(u)], jnp.concatenate(parts, axis=0), preferred_element_type=F32)

        return block

    def lift_block(u):
        def block(j):
            both = jnp.concatenate([wo[2 * j], wo[2 * j + 1]], axis=1)
            return jnp.dot(hidden[half(u), :128], both, preferred_element_type=F32)

        return block

    def set_first(u):
        def finish(total):
            first[half(u)] = (xin[half(u)].astype(F32) + 0.5 * total).astype(BF16)

        return finish

    def set_second(u):
        def finish(total):
            second[half(u)] = (first[half(u)].astype(F32) + opened[half(u)] * total).astype(BF16)

        return finish

    def set_out(u):
        def finish(total):
            out_ref[half(u)] = (second[half(u)].astype(F32) + 0.5 * total).astype(BF16)

        return finish

    def mix(u):
        weights = jnp.concatenate([wpg[t] for t in range(3)], axis=1)
        sums = jnp.dot(whole(1, u), weights, preferred_element_type=F32)
        scale = factors[1, u]
        for s in range(2):
            logit = scale * sums[:, (1 + s) * 128:(2 + s) * 128]
            opened[half(u), s * 128:(s + 1) * 128] = 1.0 / (1.0 + jnp.exp(-logit))
        pooling[16 + u * part_rows:16 + (u + 1) * part_rows] = (scale * sums[:, :128]).astype(BF16).astype(F32)
        if u == 0:
            pooling[:16] = jnp.zeros((16, 128), F32)
        size = part_rows + 16
        values = pooling[u * part_rows:u * part_rows + size]
        position = lax.broadcasted_iota(jnp.int32, (size, 128), 0) + (u * part_rows - 16)
        window_id = lax.rem(tp, 4)
        running = values
        chosen = values
        for w in range(4):
            span = 1 << w
            running = running + pltpu.roll(running, span, 0)
            counts = jnp.clip(position + 1, 1, 2 * span).astype(F32)
            chosen = jnp.where(window_id == w, running / counts, chosen)
        trail = (chosen - values)[16:].astype(BF16)
        mixed = jnp.dot(trail, mixw[0], preferred_element_type=F32)
        hidden[half(u), :128] = (mixed * pscale[...]).astype(BF16)

    def layer(u):
        yield from rs(0, u, down_block(u), set_first(u))
        yield from ag(1, u, first[half(u)])
        mix(u)
        yield from rs(1, u, lift_block(u), set_second(u))
        yield from ag(2, u, second[half(u)])
        for t in range(3):
            gu(2, u, t)
        yield from rs(2, u, down_block(u), set_out(u))

    def advance(steps):
        for step in steps:
            next(step, None)

    def send_own(ks):
        for k in ks:
            for direction in range(2):
                z_send(k, direction, 0)

    for copy in local[:early]:
        copy.wait()
    send_own(gu_ks)
    inputs = [ag(0, u, xin[half(u)]) for u in range(2)]
    advance(inputs)
    for copy in local[early:]:
        copy.wait()
    for step in range(1, half_n + 1):
        if step == half_n:
            send_own(down_ks)
        z_step(gu_ks, step)
        if step > 1:
            advance(inputs)
    todo = [(u, t) for u in range(2) for t in range(3)]
    for step in range(1, half_n + 1):
        if step == half_n - 1:
            send_own(mix_ks)
        z_step(down_ks, step)
        if step == 4:
            y_wait_all(0)
            y_wait_all(1)
        if step >= 4:
            count = 2 if step == half_n else 1
            for u, t in todo[:count]:
                gu(0, u, t)
            todo = todo[count:]
    mix_steps = list(range(1, half_n + 1))

    def mix_step():
        if mix_steps:
            z_step(mix_ks, mix_steps.pop(0))

    mix_step()
    y_wait_all(2)
    mix_step()
    halves = [layer(u) for u in range(2)]
    for turn_number in range(24):
        advance(halves)
        mix_step()
    for copy in sent:
        copy.wait_send()


def per_device(n, tpn, *arrays):
    x, gate = arrays[0], arrays[2]
    rows, width = x.shape
    kdim, ff = gate.shape
    third = ff // 3
    part = rows // 2
    vmem = pltpu.VMEM
    dma = pltpu.SemaphoreType.DMA
    half_n = n // 2
    any_spec = pl.BlockSpec(memory_space=pl.ANY)
    return pl.pallas_call(
        functools.partial(kernel, n),
        out_shape=jax.ShapeDtypeStruct((rows, width), BF16),
        in_specs=[any_spec] * len(arrays),
        out_specs=pl.BlockSpec(memory_space=pltpu.VMEM),
        scratch_shapes=[
            vmem((rows, width), BF16),
            vmem((3, 1, width), BF16),
            vmem((1, 128, 128), BF16),
            vmem((1, 128), F32),
            vmem((2, 3, n * kdim, third), BF16),
            vmem((3, 2, n, third // 2, 128), BF16),
            vmem((3, n * kdim, 128), BF16),
            vmem((n, 128, 128), BF16),
            vmem((3, 2, tpn, part, width), BF16),
            vmem((3, 2, tpn, 8, 128), F32),
            vmem((3, 2, 2, 8, 128), F32),
            vmem((3, 2, part, 128), F32),
            vmem((rows, ff), BF16),
            vmem((2, part, third), F32),
            vmem((rows, width), F32),
            vmem((rows + 16, 128), F32),
            vmem((rows, width), BF16),
            vmem((rows, width), BF16),
            vmem((3, 2, 4, part, width), BF16),
            vmem((3, 2, 4, part, width), BF16),
            vmem((3, 2, 3, part, width), BF16),
            vmem((3, 2, 2, part // 2, width), BF16),
            vmem((3, 2, 2, part, width), BF16),
            vmem((2, 2, part // 2, width), F32),
            vmem((2, part, width), F32),
            dma((24,)),
            dma((10, 2, half_n)),
            dma((10, 2, half_n)),
            dma((3, n)),
            dma((3, n)),
            dma((3, 2, 13)),
            dma((3, 2, 13)),
            dma((3, 2, tpn)),
            dma((3, 2, tpn)),
            dma((3, 2, 10)),
            dma((3, 2, 10)),
        ],
        compiler_params=pltpu.CompilerParams(
            collective_id=0, has_side_effects=True, vmem_limit_bytes=60 * 1024 * 1024
        ),
    )(*arrays)


def solution(mesh):
    return jax.shard_map(
        functools.partial(per_device, mesh.shape["fs"], mesh.shape["tp"]),
        mesh=mesh,
        in_specs=(
            P(("grp", "fs"), "tp"),
            P(None, "tp"),
            P("fs", "tp"),
            P("fs", "tp"),
            P("tp", "fs"),
            P(None, "tp"),
            P("fs", "tp"),
            P("fs", "tp"),
            P("tp", None, None),
            P(None, "tp"),
            P("tp", "fs"),
            P(None, "tp"),
        ),
        out_specs=P(("grp", "fs"), "tp"),
        check_vma=False,
    )
```
